32 devices in a mesh: fs: 16 (over z, y, x), tp: 2 (over core).
Axes of the slice: x: 2, y: 2, z: 4, core: 2. Of those that a mesh axis runs over, the one named last changes fastest.
Arguments:
- tokens: bfloat16 [2048, 2048], P('fs', 'tp'), may hold values from -300 to 300
- norm_gain: float32 [2048], P('fs'), may hold values from 0.1 to 1.9
- gate_weight: float32 [16, 2048, 1024], P(None, 'fs', 'tp'), may hold values from -1.3258252 to 1.3258252
- up_weight: float32 [16, 2048, 1024], P(None, 'fs', 'tp'), may hold values from -1.3258252 to 1.3258252
- down_weight: float32 [16, 1024, 2048], P(None, 'fs', 'tp'), may hold values from -0.1875 to 0.1875
- routes: int32 [2048, 4], P('fs'), may hold values from 0 to 15, all different within a row; in each aligned block of 128 rows (0 to 127, 128 to 255, ...) at most 64 rows name the same one
- route_weights: float32 [2048, 4], P('fs'), may hold values from 0.05 to 1
Outputs:
- mixed: bfloat16 [2048, 2048], P('fs', 'tp')
- gate_ready: bfloat16 [16, 2048, 1024], P('fs', None, 'tp')
- up_ready: bfloat16 [16, 2048, 1024], P('fs', None, 'tp')
- down_ready: bfloat16 [16, 1024, 2048], P('fs', None, 'tp')
The draws below stay inside these ranges and needn't reach their ends.
Inputs may be any that keep to these rules, and one draw needn't show every extreme that they name: `routes`: each row names 4 different experts. In each aligned block of 128 rows no expert is named more than 64 times, a bound that some block reaches.
All inputs are finite; a program needn't handle non-finite values.
Results may differ from the reference program's by a relative error of at most 0.0089.
Values may be sent and summed in bfloat16 or wider, within the bound.
A program may use at most 64 MiB of HBM per device.

```python
import math
import jax
import jax.numpy as jnp
import numpy as np
from jax import lax

D = 2048
FF = 1024
TOP_K = 4
TOK_DEV = 128
EXPERTS = 16
CAP = 64
TOKENS = 2048
N_FS = 16


def expert_matrix(key, salt):
    base = jax.random.fold_in(key, salt)
    noise = jax.random.truncated_normal(jax.random.fold_in(base, 1), -6.0, 6.0, (EXPERTS, D, FF), jnp.float32)
    column = jnp.exp(jax.random.uniform(jax.random.fold_in(base, 2), (EXPERTS, 1, FF), jnp.float32, math.log(0.5), math.log(3.0)))
    return noise * column * D ** (-0.5)


def draw_gate_weight(key, part):
    return expert_matrix(key, 11)


def draw_up_weight(key, part):
    return expert_matrix(key, 12)


def draw_tokens(key, part):
    base = jax.random.fold_in(key, 21)
    rough = jnp.exp(jax.random.uniform(jax.random.fold_in(base, 3), (1, D), jnp.float32, -0.35, 0.35))
    rising = 3.0 ** (jnp.arange(D, dtype=jnp.float32)[None, :] / max(D - 1, 1))
    noise = jax.random.truncated_normal(jax.random.fold_in(base, 1), -6.0, 6.0, (TOKENS, D), jnp.float32)
    scales = jnp.exp(jax.random.uniform(jax.random.fold_in(base, 2), (TOKENS, 1), jnp.float32, 0.0, math.log(10.0)))
    return (noise * scales * rising * rough).astype(jnp.bfloat16)


def block_levels(rng, dims, split, smallest, largest):
    loudness = 1.0
    for axis_at, shards_of in split:
        draws = jax.random.uniform(jax.random.fold_in(jax.random.fold_in(rng, 6), axis_at), (shards_of,), jnp.float32, smallest / len(split), largest / len(split))
        loudness = loudness * jnp.repeat(jnp.exp(draws), dims[axis_at] // shards_of).reshape((-1,) + (1,) * (len(dims) - 1 - axis_at))
    return loudness


def assign_block(key, own, number, rows, count, top, bound, skew):
    sequence = jax.random.permutation(key, count)
    packed, ordinary = load_shares(count, rows * top, bound, skew, True), load_shares(count, rows * top, bound, skew, False)
    places = jnp.arange(count)

    def named(sizes, turn):
        used = int((sizes > 0).sum())
        fixed = max(1, used // 4)
        shifted = fixed + (places - fixed + turn * (used - fixed)) % max(1, count - fixed)
        return jnp.zeros((count,), jnp.int32).at[sequence[jnp.where(places < fixed, places, shifted)]].set(jnp.asarray(sizes, jnp.int32))

    sizes = jnp.where(number % 4 == 0, named(packed, number // 4), named(ordinary, number - number // 4 - 1))
    mixed = jax.random.permutation(jax.random.fold_in(own, 3), count)
    source_of, receiver = mixed[0:count // 2 * 2:2], mixed[1:count // 2 * 2:2]
    slack = jnp.minimum(sizes[source_of] - 1, bound - sizes[receiver]) // 2
    slack = jnp.where((source_of == sequence[0]) | (receiver == sequence[0]) | (sizes[receiver] == 0), 0, jnp.maximum(slack, 0))
    shifted = jax.random.randint(jax.random.fold_in(own, 4), (count // 2,), 0, 1 << 20) % (slack + 1)
    sizes = sizes.at[source_of].add(-shifted).at[receiver].add(shifted)
    members = jnp.searchsorted(jnp.cumsum(sizes), jnp.arange(rows * top), side="right").astype(jnp.int32)
    table = members.reshape(top, rows).T
    table = table[jax.random.permutation(jax.random.fold_in(own, 1), rows)]
    turn = jax.random.randint(jax.random.fold_in(own, 2), (rows, 1), 0, top)
    return jnp.take_along_axis(table, (jnp.arange(top)[None, :] + turn) % top, axis=1)


def load_shares(number_of, total, limit, skew, full):
    weights = [(1 << 20) // math.isqrt(rank ** skew) + 1 for rank in range(1, number_of + 1)]
    largest = limit if full else min(limit, max(-(-total // number_of), total * weights[0] // sum(weights)))
    least = 1 if total - largest >= number_of - 1 else 0
    given, rest = [largest] + [least] * (number_of - 1), total - largest - least * (number_of - 1)
    while rest > 0:
        movable = [i for i in range(1, number_of) if given[i] < largest] or [i for i in range(1, number_of) if given[i] < limit]
        pool, budget = sum([weights[i] for i in movable]), rest
        for i in movable:
            more = min(limit - given[i], max(1, budget * weights[i] // pool), rest)
            given[i] = given[i] + more
            rest = rest - more
    return np.array(given)


def gaussian(key, extent, width, bound, cuts=(), held_as=jnp.bfloat16):
    factor_of = block_levels(key, extent, cuts, -0.22, 0.18) if cuts else 1.0
    entries = jax.random.normal(key, extent, jnp.float32) * width * factor_of
    return jnp.minimum(jnp.maximum(entries, -bound), bound).astype(held_as)


def setup_inputs(seed: int = 0) -> dict:
    splits = jax.random.split(jax.random.key(seed), 8)
    tokens = draw_tokens(jax.random.fold_in(splits[7], 71), 0)
    norm_gain = jnp.clip(1.0 + 0.18 * jax.random.normal(splits[1], (D,), jnp.float32), 0.1, 1.9)
    gate_weight = draw_gate_weight(jax.random.fold_in(splits[7], 71), 0)
    up_weight = draw_up_weight(jax.random.fold_in(splits[7], 71), 0)
    down_weight = gaussian(splits[4], (EXPERTS, FF, D), FF ** -0.5, 0.1875, ((1, 16), (2, 2)), jnp.float32)
    routes_keys = jax.random.split(jax.random.fold_in(splits[5], 1), TOKENS // TOK_DEV)
    routes_turns = jax.random.permutation(jax.random.fold_in(splits[5], 3), TOKENS // TOK_DEV)
    routes = jax.vmap(lambda own, number: assign_block(jax.random.fold_in(splits[5], 2), own, number, TOK_DEV, EXPERTS, TOP_K, CAP, 2))(routes_keys, routes_turns).reshape((TOKENS, TOP_K))
    route_weights = jnp.clip(jnp.exp(math.log(1.0) - 2.9957323 * jax.random.uniform(splits[6], (TOKENS, TOP_K), jnp.float32) ** block_levels(splits[6], (TOKENS, TOP_K), ((0, 16),), -0.2, 0.2)), 0.05, 1.0)
    return {"tokens": tokens, "norm_gain": norm_gain, "gate_weight": gate_weight, "up_weight": up_weight, "down_weight": down_weight, "routes": routes, "route_weights": route_weights}


epsilon = 1e-05

def activate(gate_pre, up_pre):
    gated = jnp.minimum(gate_pre, 7.0)
    upper = jnp.clip(up_pre, -7.0, 7.0)
    return (upper + 1.0) * gated * jax.nn.sigmoid(1.702 * gated)

def reference(tokens, norm_gain, gate_weight, up_weight, down_weight, routes, route_weights):
    gate_ready = (norm_gain[None, :, None] * gate_weight).astype(jnp.bfloat16)
    up_ready = (norm_gain[None, :, None] * up_weight).astype(jnp.bfloat16)
    down_ready = down_weight.astype(jnp.bfloat16)
    values = tokens.astype(jnp.float32)
    normed = (values * lax.rsqrt(lax.optimization_barrier(jnp.mean(values * values, axis=1, keepdims=True)) + epsilon)).astype(jnp.bfloat16)
    pairs = TOK_DEV * TOP_K
    chosen = routes.reshape(N_FS, pairs)
    onehot = (chosen[:, :, None] == jnp.arange(EXPERTS, dtype=jnp.int32)[None, None, :]).astype(jnp.int32)
    position = lax.optimization_barrier(jnp.sum(jnp.cumsum(onehot, axis=1) * onehot, axis=2)) - 1
    source = jnp.arange(N_FS, dtype=jnp.int32)[:, None]
    row_index = (source * CAP + position).astype(jnp.int32)
    token_index = (source * TOK_DEV + jnp.arange(pairs, dtype=jnp.int32)[None, :] // TOP_K).astype(jnp.int32)
    table = jnp.zeros((EXPERTS, N_FS * CAP), jnp.int32).at[chosen, row_index].set(token_index)

    def expert(operands):
        indices, gate_mat, up_mat, down_mat = operands
        rows = normed[indices]
        gate_pre = jnp.dot(rows, gate_mat, preferred_element_type=jnp.float32)
        up_pre = jnp.dot(rows, up_mat, preferred_element_type=jnp.float32)
        hidden = activate(gate_pre, up_pre).astype(jnp.bfloat16)
        return jnp.dot(hidden, down_mat, preferred_element_type=jnp.float32).astype(jnp.bfloat16)
    outputs = lax.map(expert, (table, gate_ready, up_ready, down_ready))
    picked = outputs[chosen, row_index].astype(jnp.float32).reshape(TOKENS, TOP_K, D)
    mixed = lax.optimization_barrier(jnp.sum(picked * route_weights[:, :, None], axis=1)).astype(jnp.bfloat16)
    return (mixed, gate_ready, up_ready, down_ready)
```

```python
import functools
import math

import jax
import jax.numpy as jnp
from jax import lax
from jax.experimental import pallas as pl
from jax.experimental.pallas import tpu as pltpu
from jax.sharding import PartitionSpec as P

epsilon = 1e-05
MESH = pl.DeviceIdType.MESH
CHUNKS = 4
PIECES = 4
WINDOW = 3


def activate(gate_pre, up_pre):
    gated = jnp.minimum(gate_pre, 7.0)
    upper = jnp.clip(up_pre, -7.0, 7.0)
    return (upper + 1.0) * gated * jax.nn.sigmoid(1.702 * gated)


def plane_size(n):
    return max(size for size in range(1, math.isqrt(n) + 1) if n % size == 0 and (n // size) % 2 == 0)


def kernel(
    n, cores, items, pieces, chunks,
    tokens_in, gain_in, gate_in, up_in, down_in, routes_in, weights_in,
    mixed_out, gate_out, up_out, down_out,
    tok_raw, gain_row, gain_tile, routes_v, weights_v, square,
    gate_f, up_f, down_f, gate_s, up_s, down_s, gate, up, down,
    block, info, mix_high, mix_low, picked, rows, hidden,
    results, back, part_f, part_s, lead_in, half_in, cross, cross_in, mixed,
    load_sem, w_send, w_recv, t_send, near_recv, far_recv, fwd_send, p_sem, tp_send, tp_recv,
    r_send, r_recv, h_send, h_recv, l_send, l_recv, x_send, x_recv, out_sem,
):
    me = lax.axis_index("fs")
    core = lax.axis_index("tp")
    plane = plane_size(n)
    depths = n // plane
    half = depths // 2
    z = me // plane
    q = lax.rem(me, plane)
    base = (z // half) * half
    other = half - base
    leader = half - 1 + z // half
    other_leader = half - z // half
    place_in_half = z - base

    tok_rows, width = tokens_in.shape
    depth, columns = gate_in.shape[1:]
    units = down_in.shape[1]
    piece = depth // pieces
    chunk = width // chunks
    top_count = routes_in.shape[0]

    def fs(index):
        return {"fs": index}

    def remote(source, landing, sent, received, where):
        pltpu.make_async_remote_copy(
            src_ref=source, dst_ref=landing, send_sem=sent, recv_sem=received,
            device_id=where, device_id_type=MESH,
        ).start()

    def drain(ref, semaphore):
        pltpu.make_async_copy(ref, ref, semaphore).wait()

    small = ((tokens_in, tok_raw), (gain_in, gain_row), (routes_in, routes_v), (weights_in, weights_v))
    loads = [pltpu.make_async_copy(source, landing, load_sem.at[i]) for i, (source, landing) in enumerate(small)]
    phases = []
    for source, staged, sent, landing in ((gate_in, gate_f, gate_s, gate), (up_in, up_f, up_s, up)):
        for p in range(pieces):
            phases.append((
                source.at[:, pl.ds(p * piece, piece)], staged.at[p], sent.at[p],
                landing, depth, p * piece, piece, True,
            ))
    for c in range(chunks):
        phases.append((
            down_in.at[:, :, pl.ds(c * chunk, chunk)], down_f.at[c], down_s.at[c],
            down.at[c], units, 0, units, False,
        ))
    weight_loads = [
        pltpu.make_async_copy(phase[0], phase[1], load_sem.at[len(small) + i]) for i, phase in enumerate(phases)
    ]
    loads[1].start()
    weight_loads[0].start()
    for at in (0, 2, 3):
        loads[at].start()
    for copy in weight_loads[1:]:
        copy.start()

    barrier = pltpu.get_barrier_semaphore()

    def greet(step, carry):
        pl.semaphore_signal(barrier, inc=1, device_id=fs(lax.rem(me + step, n)), device_id_type=MESH)
        return carry

    lax.fori_loop(1, n, greet, 0)
    for step in range(1, cores):
        pl.semaphore_signal(barrier, inc=1, device_id={"tp": lax.rem(core + step, cores)}, device_id_type=MESH)

    loads[1].wait()
    row_at = lax.broadcasted_iota(jnp.int32, (depth, depth), 0)
    lane_at = lax.broadcasted_iota(jnp.int32, (depth, depth), 1)
    spread = jnp.where(row_at == lane_at, jnp.broadcast_to(gain_row[...], (depth, depth)), 0.0)
    gain_tile[...] = jnp.broadcast_to(jnp.sum(spread, axis=1, keepdims=True), gain_tile.shape)

    def cast(index):
        _, staged, sent, landing, stride, offset, size, scaled = phases[index]
        weight_loads[index].wait()

        def rounded(peer):
            value = staged[peer]
            if scaled:
                lanes = gain_tile.shape[1]
                gain = gain_tile[offset:offset + size, :]
                value = value * jnp.concatenate([gain] * (value.shape[1] // lanes), axis=1)
            return value.astype(jnp.bfloat16)

        def one(step, carry):
            peer = lax.rem(me + step, n)
            sent[peer] = rounded(peer)
            return carry

        lax.fori_loop(1, n, one, 0)
        landing[pl.ds(pl.multiple_of(me * stride + offset, size), size), :] = rounded(me)

    def send(index):
        _, _, sent, landing, stride, offset, size, _ = phases[index]

        def one(step, carry):
            peer = lax.rem(me + step, n)
            remote(
                sent.at[peer], landing.at[pl.ds(pl.multiple_of(me * stride + offset, size), size)],
                w_send.at[index], w_recv.at[index], fs(peer),
            )
            return carry

        lax.fori_loop(1, n, one, 0)

    def arrive(index):
        _, _, _, landing, _, _, size, _ = phases[index]
        drain(landing.at[pl.ds(0, (n - 1) * size)], w_recv.at[index])
        if index + WINDOW < len(phases):
            send(index + WINDOW)

    def swap(buffer, slot):
        copies = []
        for step in range(1, cores):
            copies.append(
                pltpu.make_async_remote_copy(
                    src_ref=buffer.at[core], dst_ref=buffer.at[core],
                    send_sem=tp_send.at[slot, step - 1], recv_sem=tp_recv.at[slot, step - 1],
                    device_id={"tp": lax.rem(core + step, cores)}, device_id_type=MESH,
                )
            )
        for copy in copies:
            copy.start()
        return copies

    cast(0)
    loads[0].wait()
    values = tok_raw[...].astype(jnp.float32)
    square[core] = jnp.broadcast_to(jnp.sum(values * values, axis=1, keepdims=True), square.shape[1:])
    pl.semaphore_wait(barrier, n - 1 + cores - 1)
    send(0)
    swapped = swap(square, 0)

    loads[2].wait()
    loads[3].wait()
    names = lax.broadcasted_iota(jnp.int32, (n, tok_rows), 0)
    weight = jnp.zeros((n, tok_rows), jnp.float32)
    member = jnp.zeros((n, tok_rows), jnp.float32)
    for k in range(top_count):
        hit = jnp.broadcast_to(routes_v[k:k + 1, :], (n, tok_rows)) == names
        weight = weight + jnp.where(hit, jnp.broadcast_to(weights_v[k:k + 1, :], (n, tok_rows)), 0.0)
        member = member + jnp.where(hit, 1.0, 0.0)
    before = lax.broadcasted_iota(jnp.int32, (tok_rows, tok_rows), 0)
    after = lax.broadcasted_iota(jnp.int32, (tok_rows, tok_rows), 1)
    earlier = jnp.where(before < after, 1.0, 0.0).astype(jnp.bfloat16)
    place = jnp.dot(member.astype(jnp.bfloat16), earlier, preferred_element_type=jnp.float32)
    place = jnp.where(member > 0.0, place, -1.0)
    for p in range(depths):
        info[z, 0, p] = weight[p * plane:(p + 1) * plane]
        info[z, 1, p] = place[p * plane:(p + 1) * plane]

    for copy in swapped:
        copy.wait()
    total = square[0]
    for part in range(1, cores):
        total = total + square[part]
    scale = lax.rsqrt(total / (width * cores) + epsilon)
    values = tok_raw[...].astype(jnp.float32)
    lanes = scale.shape[1]
    block[z] = (values * jnp.concatenate([scale] * (width // lanes), axis=1)).astype(jnp.bfloat16)

    def give_tokens(dest, received):
        remote(block.at[z], block.at[z], t_send.at[0], received.at[0], fs(dest * plane + q))
        remote(info.at[z], info.at[z], t_send.at[1], received.at[1], fs(dest * plane + q))

    give_tokens(other_leader, far_recv)
    for step in range(1, half):
        give_tokens(base + lax.rem(place_in_half + step, half), near_recv)
    for index in range(1, min(WINDOW, len(phases))):
        cast(index)
        send(index)
    for index in range(WINDOW, len(phases)):
        cast(index)

    def take_far():
        drain(block.at[pl.ds(0, half)], far_recv.at[0])
        drain(info.at[pl.ds(0, half)], far_recv.at[1])

    def forward():
        @pl.when(z == leader)
        def _():
            take_far()
            for step in range(1, half):
                dest = fs((base + lax.rem(place_in_half + step, half)) * plane + q)
                remote(block.at[pl.ds(other, half)], block.at[pl.ds(other, half)], fwd_send.at[0], far_recv.at[0], dest)
                remote(info.at[pl.ds(other, half)], info.at[pl.ds(other, half)], fwd_send.at[1], far_recv.at[1], dest)

    own_pick = pltpu.make_async_copy(picked.at[q], rows.at[core, q], p_sem.at[2])

    def dispatch():
        @pl.when(z != leader)
        def _():
            take_far()

        if half > 1:
            drain(block.at[pl.ds(0, half - 1)], near_recv.at[0])
            drain(info.at[pl.ds(0, half - 1)], near_recv.at[1])
        slot = lax.broadcasted_iota(jnp.int32, (items, tok_rows), 0).astype(jnp.float32)

        def one(source, carry):
            weights = info[source, 0, z]
            places = info[source, 1, z]
            chosen, mixing = [], []
            for j in range(plane):
                at = jnp.broadcast_to(places[j:j + 1, :], (items, tok_rows)) == slot
                chosen.append(jnp.where(at, 1.0, 0.0))
                mixing.append(jnp.where(at, jnp.broadcast_to(weights[j:j + 1, :], (items, tok_rows)), 0.0))
            picks = jnp.concatenate(chosen, axis=0).astype(jnp.bfloat16)
            outbound = jnp.dot(picks, block[source], preferred_element_type=jnp.float32).astype(jnp.bfloat16)
            for j in range(plane):
                picked[j, source] = outbound[j * items:(j + 1) * items]
            mix = jnp.concatenate(mixing, axis=0).T
            high = mix.astype(jnp.bfloat16)
            mix_high[source] = high
            mix_low[source] = (mix - high.astype(jnp.float32)).astype(jnp.bfloat16)
            return carry

        lax.fori_loop(0, depths, one, 0)
        for step in range(1, plane):
            peer = lax.rem(q + step, plane)
            remote(picked.at[peer], rows.at[core, q], p_sem.at[0], p_sem.at[1], fs(z * plane + peer))
        own_pick.start()

    swaps = []

    def collect():
        drain(rows.at[core, pl.ds(0, plane - 1)], p_sem.at[1])
        own_pick.wait()
        swaps.extend(swap(rows, 1))

    first = 2 * pieces
    tasks = {}
    for at, task in ((0, forward), (1, dispatch), (3, collect)):
        tasks.setdefault(min(at, first - 1), []).append(task)
    outs = []
    for index in range(first):
        arrive(index)
        for task in tasks.get(index, ()):
            task()
        if index == pieces - 1:
            outs.append(pltpu.make_async_copy(gate, gate_out, out_sem.at[0]))
            outs[-1].start()
        if index == first - 1:
            outs.append(pltpu.make_async_copy(up, up_out, out_sem.at[1]))
            outs[-1].start()
    for copy in swaps:
        copy.wait()

    tile = depths * items

    def first_layer(group, carry):
        gate_pre = jnp.zeros((tile, columns), jnp.float32)
        up_pre = jnp.zeros((tile, columns), jnp.float32)
        for part in range(cores):
            taken = rows[part, group].reshape(tile, width)
            span = pl.ds(part * width, width)
            gate_pre = gate_pre + jnp.dot(taken, gate[span, :], preferred_element_type=jnp.float32)
            up_pre = up_pre + jnp.dot(taken, up[span, :], preferred_element_type=jnp.float32)
        hidden[core, group] = activate(gate_pre, up_pre).astype(jnp.bfloat16)
        return carry

    lax.fori_loop(0, plane, first_layer, 0)
    for copy in swap(hidden, 2):
        copy.wait()

    def expert(c):
        arrive(first + c)
        outs.append(pltpu.make_async_copy(down.at[c], down_out.at[:, pl.ds(c * chunk, chunk)], out_sem.at[2 + c]))
        outs[-1].start()

        def second_layer(group):
            summed = jnp.zeros((tile, chunk), jnp.float32)
            for part in range(cores):
                summed = summed + jnp.dot(
                    hidden[part, group], down[c, pl.ds(part * columns, columns), :], preferred_element_type=jnp.float32
                )
            return summed.astype(jnp.bfloat16).reshape(depths, items, chunk)

        def one(step, carry):
            peer = lax.rem(q + step, plane)
            results[c, peer] = second_layer(peer)
            remote(results.at[c, peer], back.at[c, q], r_send.at[c], r_recv.at[c], fs(z * plane + peer))
            return carry

        lax.fori_loop(1, plane, one, 0)
        back[c, q] = second_layer(q)

    def relay(c):
        drain(back.at[c, pl.ds(0, plane - 1)], r_recv.at[c])

        def one(step, carry):
            target = lax.rem(z + 1 + step, depths)
            data = back[c, :, target].reshape(plane * items, chunk)
            summed = jnp.dot(mix_high[target], data, preferred_element_type=jnp.float32)
            summed = summed + jnp.dot(mix_low[target], data, preferred_element_type=jnp.float32)
            part_f[c, target] = summed
            part_s[c, target] = summed.astype(jnp.bfloat16)
            return carry

        lax.fori_loop(0, depths, one, 0)

        @pl.when(z != leader)
        def _():
            remote(
                part_s.at[c, pl.ds(other, half)], lead_in.at[c, place_in_half],
                l_send.at[c], l_recv.at[c], fs(leader * plane + q),
            )

        for step in range(1, half):
            target = base + lax.rem(place_in_half + step, half)
            remote(
                part_s.at[c, target], half_in.at[c, place_in_half],
                h_send.at[c], h_recv.at[c], fs(target * plane + q),
            )

    def lead(c):
        @pl.when(z == leader)
        def _():
            if half > 1:
                drain(lead_in.at[c, pl.ds(0, half - 1)], l_recv.at[c])
            for k in range(half):
                summed = part_f[c, other + k]
                for step in range(1, half):
                    summed = summed + lead_in[c, lax.rem(place_in_half + step, half), k].astype(jnp.float32)
                cross[c, k] = summed.astype(jnp.bfloat16)
            for k in range(half):
                remote(cross.at[c, k], cross_in.at[c], x_send.at[c], x_recv.at[c], fs((other + k) * plane + q))

    def finish(c):
        summed = part_f[c, z]
        if half > 1:
            drain(half_in.at[c, pl.ds(0, half - 1)], h_recv.at[c])
            for step in range(1, half):
                summed = summed + half_in[c, lax.rem(place_in_half + step, half)].astype(jnp.float32)
        drain(cross_in.at[c], x_recv.at[c])
        summed = summed + cross_in[c].astype(jnp.float32)
        mixed[:, c * chunk:(c + 1) * chunk] = summed.astype(jnp.bfloat16)

    expert(0)
    for c in range(1, chunks):
        relay(c - 1)
        lead(c - 1)
        expert(c)
        finish(c - 1)
    relay(chunks - 1)
    lead(chunks - 1)
    finish(chunks - 1)
    last = pltpu.make_async_copy(mixed, mixed_out, out_sem.at[2 + chunks])
    last.start()

    for index, phase in enumerate(phases):
        _, _, sent, _, _, _, _, _ = phase
        drain(sent.at[pl.ds(0, n - 1)], w_send.at[index])
    drain(block.at[pl.ds(0, half)], t_send.at[0])
    drain(info.at[pl.ds(0, half)], t_send.at[1])
    drain(picked.at[pl.ds(0, plane - 1)], p_sem.at[0])
    for c in range(chunks):
        drain(results.at[c, pl.ds(0, plane - 1)], r_send.at[c])
        if half > 1:
            drain(part_s.at[c, pl.ds(0, half - 1)], h_send.at[c])

    @pl.when(z == leader)
    def _():
        for step in range(1, half):
            drain(block.at[pl.ds(0, half)], fwd_send.at[0])
            drain(info.at[pl.ds(0, half)], fwd_send.at[1])
        for c in range(chunks):
            drain(cross.at[c], x_send.at[c])

    @pl.when(z != leader)
    def _():
        for c in range(chunks):
            drain(part_s.at[c, pl.ds(0, half)], l_send.at[c])

    for copy in outs:
        copy.wait()
    last.wait()


def shards(n, cores, tokens, norm_gain, gate_weight, up_weight, down_weight, routes, route_weights):
    experts, depth, columns = gate_weight.shape
    units, width = down_weight.shape[1:]
    tok_rows, top_count = routes.shape
    items = 2 * tok_rows * top_count // experts
    plane = plane_size(n)
    depths = n // plane
    half = depths // 2
    pieces = max(1, min(PIECES, depth // 32))
    piece = depth // pieces
    chunk = max(128, width // CHUNKS)
    chunks = width // chunk
    lanes = min(128, width)
    bf16, f32, dma = jnp.bfloat16, jnp.float32, pltpu.SemaphoreType.DMA
    phases = 2 * pieces + chunks

    anywhere = pl.BlockSpec(memory_space=pl.ANY)
    mixed, gate_ready, up_ready, down_ready = pl.pallas_call(
        functools.partial(kernel, n, cores, items, pieces, chunks),
        out_shape=(
            jax.ShapeDtypeStruct((tok_rows, width), bf16),
            jax.ShapeDtypeStruct((n * depth, columns), bf16),
            jax.ShapeDtypeStruct((n * depth, columns), bf16),
            jax.ShapeDtypeStruct((n * units, width), bf16),
        ),
        in_specs=[anywhere] * 7,
        out_specs=(anywhere,) * 4,
        scratch_shapes=[
            pltpu.VMEM((tok_rows, width), bf16),
            pltpu.VMEM((1, depth), f32),
            pltpu.VMEM((depth, lanes), f32),
            pltpu.VMEM((top_count, tok_rows), jnp.int32),
            pltpu.VMEM((top_count, tok_rows), f32),
            pltpu.VMEM((cores, tok_rows, lanes), f32),
            pltpu.VMEM((pieces, n, piece, columns), f32),
            pltpu.VMEM((pieces, n, piece, columns), f32),
            pltpu.VMEM((chunks, n, units, chunk), f32),
            pltpu.VMEM((pieces, n, piece, columns), bf16),
            pltpu.VMEM((pieces, n, piece, columns), bf16),
            pltpu.VMEM((chunks, n, units, chunk), bf16),
            pltpu.VMEM((n * depth, columns), bf16),
            pltpu.VMEM((n * depth, columns), bf16),
            pltpu.VMEM((chunks, n * units, chunk), bf16),
            pltpu.VMEM((depths, tok_rows, width), bf16),
            pltpu.VMEM((depths, 2, depths, plane, tok_rows), f32),
            pltpu.VMEM((depths, tok_rows, plane * items), bf16),
            pltpu.VMEM((depths, tok_rows, plane * items), bf16),
            pltpu.VMEM((plane, depths, items, width), bf16),
            pltpu.VMEM((cores, plane, depths, items, width), bf16),
            pltpu.VMEM((cores, plane, depths * items, columns), bf16),
            pltpu.VMEM((chunks, plane, depths, items, chunk), bf16),
            pltpu.VMEM((chunks, plane, depths, items, chunk), bf16),
            pltpu.VMEM((chunks, depths, tok_rows, chunk), f32),
            pltpu.VMEM((chunks, depths, tok_rows, chunk), bf16),
            pltpu.VMEM((chunks, half, half, tok_rows, chunk), bf16),
            pltpu.VMEM((chunks, half, tok_rows, chunk), bf16),
            pltpu.VMEM((chunks, half, tok_rows, chunk), bf16),
            pltpu.VMEM((chunks, tok_rows, chunk), bf16),
            pltpu.VMEM((tok_rows, width), bf16),
            dma((4 + phases,)),
            dma((phases,)),
            dma((phases,)),
            dma((2,)),
            dma((2,)),
            dma((2,)),
            dma((2,)),
            dma((3,)),
            dma((3, max(1, cores - 1))),
            dma((3, max(1, cores - 1))),
            dma((chunks,)),
            dma((chunks,)),
            dma((chunks,)),
            dma((chunks,)),
            dma((chunks,)),
            dma((chunks,)),
            dma((chunks,)),
            dma((chunks,)),
            dma((3 + chunks,)),
        ],
        compiler_params=pltpu.CompilerParams(
            collective_id=0, has_side_effects=True, vmem_limit_bytes=58 * 1024 * 1024
        ),
    )(tokens, norm_gain.reshape(1, depth), gate_weight, up_weight, down_weight, routes.T, route_weights.T)
    return (mixed, gate_ready[None], up_ready[None], down_ready[None])


def solution(mesh):
    placed = (
        P("fs", "tp"),
        P("fs"),
        P(None, "fs", "tp"),
        P(None, "fs", "tp"),
        P(None, "fs", "tp"),
        P("fs", None),
        P("fs", None),
    )
    return jax.shard_map(
        functools.partial(shards, mesh.shape["fs"], mesh.shape["tp"]),
        mesh=mesh,
        in_specs=placed,
        out_specs=(P("fs", "tp"), P("fs", None, "tp"), P("fs", None, "tp"), P("fs", None, "tp")),
        check_vma=False,
    )
```

```python
import functools
import math

import jax
import jax.numpy as jnp
from jax import lax
from jax.experimental import pallas as pl
from jax.experimental.pallas import tpu as pltpu
from jax.sharding import PartitionSpec as P

epsilon = 1e-05
MESH = pl.DeviceIdType.MESH
CHUNKS = 8
PARTS = 4
WINDOW, LATE_WINDOW = 4, 3
RELAY_LAG, LEAD_LAG, END_LAG = 4, 6, 7
NEAR_AT, FORWARD_AT, FAR_AT, COLLECT_AT = 2, 2, 7, 12


def activate(gate_pre, up_pre):
    gated = jnp.minimum(gate_pre, 7.0)
    upper = jnp.clip(up_pre, -7.0, 7.0)
    return (upper + 1.0) * gated * jax.nn.sigmoid(1.702 * gated)


def plane_size(n):
    return max(size for size in range(1, math.isqrt(n) + 1) if n % size == 0 and (n // size) % 2 == 0)


def kernel(
    n, cores, items, parts, chunks,
    tokens_in, gain_in, gate_in, up_in, down_in, routes_in, weights_in,
    mixed, pair, down,
    tok_raw, gain_row, gain_tile, routes_v, weights_v, square,
    gate_f, up_f, down_f, pair_s, down_s,
    block, info, picks, mix_high, mix_low, picked, rows, hidden,
    results, back, part_f, part_s, lead_in, half_in, cross, cross_in,
    load_sem, w_send, w_recv, t_send, near_recv, far_recv, fwd_send, p_send, p_recv, own_sem, tp_send, tp_recv,
    r_send, r_recv, h_send, h_recv, l_send, l_recv, x_send, x_recv,
):
    me = lax.axis_index("fs")
    core = lax.axis_index("tp")
    plane = plane_size(n)
    depths = n // plane
    half = depths // 2
    z = me // plane
    q = lax.rem(me, plane)
    base = (z // half) * half
    other = half - base
    leader = half - 1 + z // half
    other_leader = half - z // half
    place_in_half = z - base

    tok_rows, width = tokens_in.shape
    depth, columns = gate_in.shape[1:]
    units = down_in.shape[1]
    pieces = pair.shape[0]
    lanes = columns // pieces
    size = depth // parts
    chunk = width // chunks
    top_count = routes_in.shape[0]

    def fs(index):
        return {"fs": index}

    def remote(source, landing, sent, received, where):
        pltpu.make_async_remote_copy(
            src_ref=source, dst_ref=landing, send_sem=sent, recv_sem=received,
            device_id=where, device_id_type=MESH,
        ).start()

    def drain(ref, semaphore):
        pltpu.make_async_copy(ref, ref, semaphore).wait()

    barrier = pltpu.get_barrier_semaphore()

    def greet(step, carry):
        pl.semaphore_signal(barrier, inc=1, device_id=fs(lax.rem(me + step, n)), device_id_type=MESH)
        return carry

    lax.fori_loop(1, n, greet, 0)
    for step in range(1, cores):
        pl.semaphore_signal(barrier, inc=1, device_id={"tp": lax.rem(core + step, cores)}, device_id_type=MESH)

    small = ((tokens_in, tok_raw), (gain_in, gain_row), (routes_in, routes_v), (weights_in, weights_v))
    loads = [pltpu.make_async_copy(source, landing, load_sem.at[i, 0]) for i, (source, landing) in enumerate(small)]
    phases = []
    for p in range(pieces):
        for r in range(parts):
            at = pl.ds(r * size, size), pl.ds(p * lanes, lanes)
            sources = ((gate_in.at[:, at[0], at[1]], gate_f.at[p, r]), (up_in.at[:, at[0], at[1]], up_f.at[p, r]))
            phases.append((sources, pair_s.at[p, r], pair.at[p], depth, r * size, size))
    for c in range(chunks):
        sources = ((down_in.at[:, :, pl.ds(c * chunk, chunk)], down_f.at[c]),)
        phases.append((sources, down_s.at[c], down.at[c], units, 0, units))
    weight_loads = []
    for phase in phases:
        at = len(small) + len(weight_loads)
        weight_loads.append([
            pltpu.make_async_copy(source, landing, load_sem.at[at, i]) for i, (source, landing) in enumerate(phase[0])
        ])
    loads[1].start()
    for copy in weight_loads[0]:
        copy.start()
    for at in (0, 2, 3):
        loads[at].start()
    for copies in weight_loads[1:]:
        for copy in copies:
            copy.start()

    loads[1].wait()
    row_at = lax.broadcasted_iota(jnp.int32, (depth, depth), 0)
    lane_at = lax.broadcasted_iota(jnp.int32, (depth, depth), 1)
    spread = jnp.where(row_at == lane_at, jnp.broadcast_to(gain_row[...], (depth, depth)), 0.0)
    gain_tile[...] = jnp.broadcast_to(jnp.sum(spread, axis=1, keepdims=True), gain_tile.shape)

    def cast(index):
        sources, sent, landing, stride, offset, rows_sent = phases[index]
        for copy in weight_loads[index]:
            copy.wait()

        def rounded(peer):
            if len(sources) == 1:
                return sources[0][1][peer].astype(jnp.bfloat16)
            gain = gain_tile[offset:offset + rows_sent, :]
            return jnp.concatenate([(staged[peer] * gain).astype(jnp.bfloat16) for _, staged in sources], axis=1)

        def one(step, carry):
            peer = lax.rem(me + step, n)
            sent[peer] = rounded(peer)
            return carry

        lax.fori_loop(1, n, one, 0)
        landing[pl.ds(pl.multiple_of(me * stride + offset, rows_sent), rows_sent), :] = rounded(me)

    def send(index):
        _, sent, landing, stride, offset, rows_sent = phases[index]

        def one(step, carry):
            peer = lax.rem(me + step, n)
            remote(
                sent.at[peer], landing.at[pl.ds(pl.multiple_of(me * stride + offset, rows_sent), rows_sent)],
                w_send.at[index], w_recv.at[index], fs(peer),
            )
            return carry

        lax.fori_loop(1, n, one, 0)

    first = pieces * parts
    issued = []

    def arrive(index):
        _, _, landing, _, _, rows_sent = phases[index]
        drain(landing.at[pl.ds(0, (n - 1) * rows_sent)], w_recv.at[index])
        ahead = index + (WINDOW if index < first else LATE_WINDOW)
        while len(issued) <= min(ahead, len(phases) - 1):
            send(len(issued))
            issued.append(len(issued))

    def swap(buffer, slot):
        copies = []
        for step in range(1, cores):
            copies.append(
                pltpu.make_async_remote_copy(
                    src_ref=buffer, dst_ref=buffer,
                    send_sem=tp_send.at[slot, step - 1], recv_sem=tp_recv.at[slot, step - 1],
                    device_id={"tp": lax.rem(core + step, cores)}, device_id_type=MESH,
                )
            )
        for copy in copies:
            copy.start()
        return copies

    cast(0)
    loads[0].wait()
    values = tok_raw[...].astype(jnp.float32)
    square[core] = jnp.broadcast_to(jnp.sum(values * values, axis=1, keepdims=True), square.shape[1:])
    pl.semaphore_wait(barrier, n - 1 + cores - 1)
    send(0)
    issued.append(0)
    swapped = swap(square.at[core], 0)

    loads[2].wait()
    loads[3].wait()
    names = lax.broadcasted_iota(jnp.int32, (n, tok_rows), 0)
    weight = jnp.zeros((n, tok_rows), jnp.float32)
    member = jnp.zeros((n, tok_rows), jnp.float32)
    for k in range(top_count):
        hit = jnp.broadcast_to(routes_v[k:k + 1, :], (n, tok_rows)) == names
        weight = weight + jnp.where(hit, jnp.broadcast_to(weights_v[k:k + 1, :], (n, tok_rows)), 0.0)
        member = member + jnp.where(hit, 1.0, 0.0)
    before = lax.broadcasted_iota(jnp.int32, (tok_rows, tok_rows), 0)
    after = lax.broadcasted_iota(jnp.int32, (tok_rows, tok_rows), 1)
    earlier = jnp.where(before < after, 1.0, 0.0).astype(jnp.bfloat16)
    place = jnp.dot(member.astype(jnp.bfloat16), earlier, preferred_element_type=jnp.float32)
    place = jnp.where(member > 0.0, place, -1.0)
    for p in range(depths):
        info[z, 0, p] = weight[p * plane:(p + 1) * plane]
        info[z, 1, p] = place[p * plane:(p + 1) * plane]

    for copy in swapped:
        copy.wait()
    total = square[0]
    for part in range(1, cores):
        total = total + square[part]
    scale = lax.rsqrt(total / (width * cores) + epsilon)
    values = tok_raw[...].astype(jnp.float32)
    scale = jnp.concatenate([scale] * (width // scale.shape[1]), axis=1)
    block[z] = (values * scale).astype(jnp.bfloat16)

    def give_tokens(dest, received):
        remote(block.at[z], block.at[z], t_send.at[0], received.at[0], fs(dest * plane + q))
        remote(info.at[z], info.at[z], t_send.at[1], received.at[1], fs(dest * plane + q))

    give_tokens(other_leader, far_recv)
    for step in range(1, half):
        give_tokens(base + lax.rem(place_in_half + step, half), near_recv)
    for index in range(1, min(WINDOW, len(phases))):
        cast(index)
        send(index)
        issued.append(index)
    for index in range(WINDOW, len(phases)):
        cast(index)

    def take_far():
        drain(block.at[pl.ds(0, half)], far_recv.at[0])
        drain(info.at[pl.ds(0, half)], far_recv.at[1])

    def forward():
        @pl.when(z == leader)
        def _():
            take_far()
            for step in range(1, half):
                dest = fs((base + lax.rem(place_in_half + step, half)) * plane + q)
                remote(block.at[pl.ds(other, half)], block.at[pl.ds(other, half)], fwd_send.at[0], far_recv.at[0], dest)
                remote(info.at[pl.ds(other, half)], info.at[pl.ds(other, half)], fwd_send.at[1], far_recv.at[1], dest)

    slices = picked.shape[0]
    slice_width = width // slices
    own_picks = [
        pltpu.make_async_copy(picked.at[f, q], rows.at[core, f, q], own_sem.at[f]) for f in range(slices)
    ]

    def choose(source):
        slot = lax.broadcasted_iota(jnp.int32, (items, tok_rows), 0).astype(jnp.float32)
        weights = info[source, 0, z]
        places = info[source, 1, z]
        chosen, mixing = [], []
        for j in range(plane):
            at = jnp.broadcast_to(places[j:j + 1, :], (items, tok_rows)) == slot
            chosen.append(jnp.where(at, 1.0, 0.0))
            mixing.append(jnp.where(at, jnp.broadcast_to(weights[j:j + 1, :], (items, tok_rows)), 0.0))
        picks[...] = jnp.concatenate(chosen, axis=0).astype(jnp.bfloat16)
        mix = jnp.concatenate(mixing, axis=0).T
        high = mix.astype(jnp.bfloat16)
        mix_high[source] = high
        mix_low[source] = (mix - high.astype(jnp.float32)).astype(jnp.bfloat16)

    def dispatch(turn, f):
        if turn < half:
            source = base + lax.rem(place_in_half + turn, half)
        else:
            source = other + (turn - half)
        if f == 0:
            if turn == 1:
                drain(block.at[pl.ds(0, half - 1)], near_recv.at[0])
                drain(info.at[pl.ds(0, half - 1)], near_recv.at[1])
            if turn == half:
                @pl.when(z != leader)
                def _():
                    take_far()
            choose(source)
        part = block[source, :, f * slice_width:(f + 1) * slice_width]
        outbound = jnp.dot(picks[...], part, preferred_element_type=jnp.float32).astype(jnp.bfloat16)
        for j in range(plane):
            picked[f, j, source] = outbound[j * items:(j + 1) * items]
        for step in range(1, plane):
            peer = lax.rem(q + step, plane)
            remote(
                picked.at[f, peer, source], rows.at[core, f, q, source],
                p_send.at[f], p_recv.at[f], fs(z * plane + peer),
            )
        if turn == depths - 1:
            own_picks[f].start()

    swaps = []

    def collect():
        for f in range(slices):
            drain(rows.at[core, f, pl.ds(0, plane - 1)], p_recv.at[f])
            own_picks[f].wait()
        swaps.extend(swap(rows.at[core], 1))

    steps = [(0, dispatch, (0, 0))]
    for turn in range(depths):
        for f in range(slices):
            if turn + f > 0:
                at = turn * slices + f if turn < half else FAR_AT + (turn - half) * slices + f
                steps.append((at, dispatch, (turn, f)))
    at_far = next(i for i, (_, _, what) in enumerate(steps) if what[0] == half)
    steps.insert(at_far, (FORWARD_AT, forward, ()))
    steps.append((COLLECT_AT, collect, ()))
    tasks = {}
    for at, task, what in steps:
        tasks.setdefault(min(at, first - 1), []).append((task, what))
    tile = depths * items

    def first_layer(p):
        def one(group, carry):
            both = jnp.zeros((tile, 2 * lanes), jnp.float32)
            for part in range(cores):
                taken = jnp.concatenate([rows[part, f, group].reshape(tile, slice_width) for f in range(slices)], axis=1)
                both = both + jnp.dot(taken, pair[p, pl.ds(part * width, width), :], preferred_element_type=jnp.float32)
            hidden[core, p, group] = activate(both[:, :lanes], both[:, lanes:]).astype(jnp.bfloat16)
            return carry

        lax.fori_loop(0, plane, one, 0)
        swaps.extend(swap(hidden.at[core, p], 2 + p))

    computed = 0
    for index in range(first):
        arrive(index)
        for task, what in tasks.get(index, ()):
            task(*what)
        if index > COLLECT_AT or index == first - 1:
            if computed == 0:
                while swaps:
                    swaps.pop().wait()
            while (computed + 1) * parts <= index + 1:
                first_layer(computed)
                computed += 1

    def expert(c):
        arrive(first + c)
        while swaps:
            swaps.pop(0).wait()

        def second_layer(group):
            summed = jnp.zeros((tile, chunk), jnp.float32)
            for part in range(cores):
                units_in = jnp.concatenate([hidden[part, p, group] for p in range(pieces)], axis=1)
                summed = summed + jnp.dot(
                    units_in, down[c, pl.ds(part * columns, columns), :], preferred_element_type=jnp.float32
                )
            return summed.astype(jnp.bfloat16).reshape(depths, items, chunk)

        def one(step, carry):
            peer = lax.rem(q + step, plane)
            results[c, peer] = second_layer(peer)
            remote(results.at[c, peer], back.at[c, q], r_send.at[c], r_recv.at[c], fs(z * plane + peer))
            return carry

        lax.fori_loop(1, plane, one, 0)
        back[c, q] = second_layer(q)

    def relay(c):
        drain(back.at[c, pl.ds(0, plane - 1)], r_recv.at[c])

        def one(step, carry):
            target = lax.rem(z + 1 + step, depths)
            data = back[c, :, target].reshape(plane * items, chunk)
            summed = jnp.dot(mix_high[target], data, preferred_element_type=jnp.float32)
            summed = summed + jnp.dot(mix_low[target], data, preferred_element_type=jnp.float32)
            part_f[c, target] = summed
            part_s[c, target] = summed.astype(jnp.bfloat16)
            return carry

        lax.fori_loop(0, depths, one, 0)

        @pl.when(z != leader)
        def _():
            remote(
                part_s.at[c, pl.ds(other, half)], lead_in.at[c, place_in_half],
                l_send.at[c], l_recv.at[c], fs(leader * plane + q),
            )

        for step in range(1, half):
            target = base + lax.rem(place_in_half + step, half)
            remote(
                part_s.at[c, target], half_in.at[c, place_in_half],
                h_send.at[c], h_recv.at[c], fs(target * plane + q),
            )

    def lead(c):
        @pl.when(z == leader)
        def _():
            if half > 1:
                drain(lead_in.at[c, pl.ds(0, half - 1)], l_recv.at[c])
            for k in range(half):
                summed = part_f[c, other + k]
                for step in range(1, half):
                    summed = summed + lead_in[c, lax.rem(place_in_half + step, half), k].astype(jnp.float32)
                cross[c, k] = summed.astype(jnp.bfloat16)
            for k in range(half):
                remote(cross.at[c, k], cross_in.at[c], x_send.at[c], x_recv.at[c], fs((other + k) * plane + q))

    def finish(c):
        summed = part_f[c, z]
        if half > 1:
            drain(half_in.at[c, pl.ds(0, half - 1)], h_recv.at[c])
            for step in range(1, half):
                summed = summed + half_in[c, lax.rem(place_in_half + step, half)].astype(jnp.float32)
        drain(cross_in.at[c], x_recv.at[c])
        summed = summed + cross_in[c].astype(jnp.float32)
        mixed[:, c * chunk:(c + 1) * chunk] = summed.astype(jnp.bfloat16)

    stages = ((relay, RELAY_LAG), (lead, LEAD_LAG), (finish, END_LAG))
    done = [0, 0, 0]
    for c in range(chunks):
        expert(c)
        for stage, (task, lag) in enumerate(stages):
            if c >= lag:
                task(done[stage])
                done[stage] += 1
    while done[0] < chunks:
        relay(done[0])
        done[0] += 1
        if done[1] < done[0] - 1:
            lead(done[1])
            done[1] += 1
    for c in range(done[1], chunks):
        lead(c)
    for c in range(done[2], chunks):
        finish(c)
    for index, phase in enumerate(phases):
        drain(phase[1].at[pl.ds(0, n - 1)], w_send.at[index])
    drain(block.at[pl.ds(0, half)], t_send.at[0])
    drain(info.at[pl.ds(0, half)], t_send.at[1])
    for f in range(slices):
        drain(picked.at[f, pl.ds(0, plane - 1)], p_send.at[f])
    for c in range(chunks):
        drain(results.at[c, pl.ds(0, plane - 1)], r_send.at[c])
        if half > 1:
            drain(part_s.at[c, pl.ds(0, half - 1)], h_send.at[c])

    @pl.when(z == leader)
    def _():
        for step in range(1, half):
            drain(block.at[pl.ds(0, half)], fwd_send.at[0])
            drain(info.at[pl.ds(0, half)], fwd_send.at[1])
        for c in range(chunks):
            drain(cross.at[c], x_send.at[c])

    @pl.when(z != leader)
    def _():
        for c in range(chunks):
            drain(part_s.at[c, pl.ds(0, half)], l_send.at[c])


def place(mixed, pair, down, mixed_out, gate_out, up_out, down_out, sem):
    pieces, _, both = pair.shape
    chunks, _, chunk = down.shape
    lanes = both // 2
    moves = [(mixed, mixed_out)]
    for p in range(pieces):
        at = pl.ds(p * lanes, lanes)
        moves.append((pair.at[p, :, pl.ds(0, lanes)], gate_out.at[:, at]))
        moves.append((pair.at[p, :, pl.ds(lanes, lanes)], up_out.at[:, at]))
    for c in range(chunks):
        moves.append((down.at[c], down_out.at[:, pl.ds(c * chunk, chunk)]))
    copies = [pltpu.make_async_copy(source, landing, sem.at[i]) for i, (source, landing) in enumerate(moves)]
    for copy in copies:
        copy.start()
    for copy in copies:
        copy.wait()


def shards(n, cores, tokens, norm_gain, gate_weight, up_weight, down_weight, routes, route_weights):
    experts, depth, columns = gate_weight.shape
    units, width = down_weight.shape[1:]
    tok_rows, top_count = routes.shape
    items = 2 * tok_rows * top_count // experts
    plane = plane_size(n)
    depths = n // plane
    half = depths // 2
    parts = max(1, min(PARTS, depth // 16))
    lanes = min(128, columns)
    pieces = columns // lanes
    chunk = max(128, width // CHUNKS)
    chunks = width // chunk
    slices = 2 if width % 256 == 0 else 1
    bf16, f32, dma = jnp.bfloat16, jnp.float32, pltpu.SemaphoreType.DMA
    phases = pieces * parts + chunks

    arrays = tokens, norm_gain.reshape(1, depth), gate_weight, up_weight, down_weight, routes.T, route_weights.T
    anywhere = pl.BlockSpec(memory_space=pl.ANY)
    near = pl.BlockSpec(memory_space=pltpu.VMEM)
    results = pl.pallas_call(
        functools.partial(kernel, n, cores, items, parts, chunks),
        out_shape=(
            jax.ShapeDtypeStruct((tok_rows, width), bf16),
            jax.ShapeDtypeStruct((pieces, n * depth, 2 * lanes), bf16),
            jax.ShapeDtypeStruct((chunks, n * units, chunk), bf16),
        ),
        in_specs=[anywhere] * 7,
        out_specs=(near,) * 3,
        scratch_shapes=[
            pltpu.VMEM((tok_rows, width), bf16),
            pltpu.VMEM((1, depth), f32),
            pltpu.VMEM((depth, lanes), f32),
            pltpu.VMEM((top_count, tok_rows), jnp.int32),
            pltpu.VMEM((top_count, tok_rows), f32),
            pltpu.VMEM((cores, tok_rows, lanes), f32),
            pltpu.VMEM((pieces, parts, n, depth // parts, lanes), f32),
            pltpu.VMEM((pieces, parts, n, depth // parts, lanes), f32),
            pltpu.VMEM((chunks, n, units, chunk), f32),
            pltpu.VMEM((pieces, parts, n, depth // parts, 2 * lanes), bf16),
            pltpu.VMEM((chunks, n, units, chunk), bf16),
            pltpu.VMEM((depths, tok_rows, width), bf16),
            pltpu.VMEM((depths, 2, depths, plane, tok_rows), f32),
            pltpu.VMEM((plane * items, tok_rows), bf16),
            pltpu.VMEM((depths, tok_rows, plane * items), bf16),
            pltpu.VMEM((depths, tok_rows, plane * items), bf16),
            pltpu.VMEM((slices, plane, depths, items, width // slices), bf16),
            pltpu.VMEM((cores, slices, plane, depths, items, width // slices), bf16),
            pltpu.VMEM((cores, pieces, plane, depths * items, lanes), bf16),
            pltpu.VMEM((chunks, plane, depths, items, chunk), bf16),
            pltpu.VMEM((chunks, plane, depths, items, chunk), bf16),
            pltpu.VMEM((chunks, depths, tok_rows, chunk), f32),
            pltpu.VMEM((chunks, depths, tok_rows, chunk), bf16),
            pltpu.VMEM((chunks, half, half, tok_rows, chunk), bf16),
            pltpu.VMEM((chunks, half, tok_rows, chunk), bf16),
            pltpu.VMEM((chunks, half, tok_rows, chunk), bf16),
            pltpu.VMEM((chunks, tok_rows, chunk), bf16),
            dma((4 + phases, 2)),
            dma((phases,)),
            dma((phases,)),
            dma((2,)),
            dma((2,)),
            dma((2,)),
            dma((2,)),
            dma((slices,)),
            dma((slices,)),
            dma((slices,)),
            dma((2 + pieces, max(1, cores - 1))),
            dma((2 + pieces, max(1, cores - 1))),
            dma((chunks,)),
            dma((chunks,)),
            dma((chunks,)),
            dma((chunks,)),
            dma((chunks,)),
            dma((chunks,)),
            dma((chunks,)),
            dma((chunks,)),
        ],
        compiler_params=pltpu.CompilerParams(
            collective_id=0, has_side_effects=True, vmem_limit_bytes=44 * 1024 * 1024
        ),
    )(*(pltpu.with_memory_space_constraint(array, pltpu.HBM) for array in arrays))
    ready = (tok_rows, width), (n * depth, columns), (n * depth, columns), (n * units, width)
    mixed, gate_ready, up_ready, down_ready = pl.pallas_call(
        place,
        out_shape=tuple(jax.ShapeDtypeStruct(shape, bf16) for shape in ready),
        in_specs=[anywhere] * 3,
        out_specs=(anywhere,) * 4,
        scratch_shapes=[dma((1 + 2 * pieces + chunks,))],
        compiler_params=pltpu.CompilerParams(vmem_limit_bytes=1024 * 1024),
    )(*results)
    return (mixed, gate_ready[None], up_ready[None], down_ready[None])


def solution(mesh):
    placed = (
        P("fs", "tp"),
        P("fs"),
        P(None, "fs", "tp"),
        P(None, "fs", "tp"),
        P(None, "fs", "tp"),
        P("fs", None),
        P("fs", None),
    )
    return jax.shard_map(
        functools.partial(shards, mesh.shape["fs"], mesh.shape["tp"]),
        mesh=mesh,
        in_specs=placed,
        out_specs=(P("fs", "tp"), P("fs", None, "tp"), P("fs", None, "tp"), P("fs", None, "tp")),
        check_vma=False,
    )
```

```python
import functools
import math

import jax
import jax.numpy as jnp
from jax import lax
from jax.experimental import pallas as pl
from jax.experimental.pallas import tpu as pltpu
from jax.sharding import PartitionSpec as P

epsilon = 1e-05
MESH = pl.DeviceIdType.MESH
CHUNKS = 8
PARTS = 4
WINDOW, LATE_WINDOW = 4, 3
RELAY_LAG, LEAD_LAG, END_LAG = 2, 4, 7
DIRECT = 1
NEAR_AT, FORWARD_AT, FAR_AT, COLLECT_AT = 2, 2, 7, 12


def activate(gate_pre, up_pre):
    gated = jnp.minimum(gate_pre, 7.0)
    upper = jnp.clip(up_pre, -7.0, 7.0)
    return (upper + 1.0) * gated * jax.nn.sigmoid(1.702 * gated)


def plane_size(n):
    return max(size for size in range(1, math.isqrt(n) + 1) if n % size == 0 and (n // size) % 2 == 0)


def kernel(
    n, cores, items, parts, chunks,
    tokens_in, gain_in, gate_in, up_in, down_in, routes_in, weights_in,
    mixed, pair, down,
    tok_raw, gain_row, gain_tile, routes_v, weights_v, square,
    gate_f, up_f, down_f, pair_s, down_s,
    block, info, picks, mix_high, mix_low, picked, rows, hidden,
    results, back, part_f, part_s, lead_in, half_in, cross, cross_in,
    load_sem, w_send, w_recv, t_send, near_recv, far_recv, fwd_send, p_send, p_recv, own_sem, tp_send, tp_recv,
    r_send, r_recv, h_send, h_recv, l_send, l_recv, x_send, x_recv,
):
    me = lax.axis_index("fs")
    core = lax.axis_index("tp")
    plane = plane_size(n)
    depths = n // plane
    half = depths // 2
    z = me // plane
    q = lax.rem(me, plane)
    base = (z // half) * half
    other = half - base
    leader = half - 1 + z // half
    other_leader = half - z // half
    place_in_half = z - base

    tok_rows, width = tokens_in.shape
    depth, columns = gate_in.shape[1:]
    units = down_in.shape[1]
    pieces = pair.shape[0]
    lanes = columns // pieces
    size = depth // parts
    chunk = width // chunks
    top_count = routes_in.shape[0]

    def fs(index):
        return {"fs": index}

    def remote(source, landing, sent, received, where):
        pltpu.make_async_remote_copy(
            src_ref=source, dst_ref=landing, send_sem=sent, recv_sem=received,
            device_id=where, device_id_type=MESH,
        ).start()

    def drain(ref, semaphore):
        pltpu.make_async_copy(ref, ref, semaphore).wait()

    barrier = pltpu.get_barrier_semaphore()

    def greet(step, carry):
        pl.semaphore_signal(barrier, inc=1, device_id=fs(lax.rem(me + step, n)), device_id_type=MESH)
        return carry

    lax.fori_loop(1, n, greet, 0)
    for step in range(1, cores):
        pl.semaphore_signal(barrier, inc=1, device_id={"tp": lax.rem(core + step, cores)}, device_id_type=MESH)

    small = ((tokens_in, tok_raw), (gain_in, gain_row), (routes_in, routes_v), (weights_in, weights_v))
    loads = [pltpu.make_async_copy(source, landing, load_sem.at[i, 0]) for i, (source, landing) in enumerate(small)]
    phases = []
    for p in range(pieces):
        for r in range(parts):
            at = pl.ds(r * size, size), pl.ds(p * lanes, lanes)
            sources = ((gate_in.at[:, at[0], at[1]], gate_f.at[p, r]), (up_in.at[:, at[0], at[1]], up_f.at[p, r]))
            phases.append((sources, pair_s.at[p, r], pair.at[p], depth, r * size, size))
    for c in range(chunks):
        sources = ((down_in.at[:, :, pl.ds(c * chunk, chunk)], down_f.at[c]),)
        phases.append((sources, down_s.at[c], down.at[c], units, 0, units))
    weight_loads = []
    for phase in phases:
        at = len(small) + len(weight_loads)
        weight_loads.append([
            pltpu.make_async_copy(source, landing, load_sem.at[at, i]) for i, (source, landing) in enumerate(phase[0])
        ])
    loads[1].start()
    for copy in weight_loads[0]:
        copy.start()
    for at in (0, 2, 3):
        loads[at].start()
    for copies in weight_loads[1:]:
        for copy in copies:
            copy.start()

    loads[1].wait()
    row_at = lax.broadcasted_iota(jnp.int32, (depth, depth), 0)
    lane_at = lax.broadcasted_iota(jnp.int32, (depth, depth), 1)
    spread = jnp.where(row_at == lane_at, jnp.broadcast_to(gain_row[...], (depth, depth)), 0.0)
    gain_tile[...] = jnp.broadcast_to(jnp.sum(spread, axis=1, keepdims=True), gain_tile.shape)

    def cast(index):
        sources, sent, landing, stride, offset, rows_sent = phases[index]
        for copy in weight_loads[index]:
            copy.wait()

        def rounded(peer):
            if len(sources) == 1:
                return sources[0][1][peer].astype(jnp.bfloat16)
            gain = gain_tile[offset:offset + rows_sent, :]
            return jnp.concatenate([(staged[peer] * gain).astype(jnp.bfloat16) for _, staged in sources], axis=1)

        def one(step, carry):
            peer = lax.rem(me + step, n)
            sent[peer] = rounded(peer)
            return carry

        lax.fori_loop(1, n, one, 0)
        landing[pl.ds(pl.multiple_of(me * stride + offset, rows_sent), rows_sent), :] = rounded(me)

    def send(index):
        _, sent, landing, stride, offset, rows_sent = phases[index]

        def one(step, carry):
            peer = lax.rem(me + step, n)
            remote(
                sent.at[peer], landing.at[pl.ds(pl.multiple_of(me * stride + offset, rows_sent), rows_sent)],
                w_send.at[index], w_recv.at[index], fs(peer),
            )
            return carry

        lax.fori_loop(1, n, one, 0)

    first = pieces * parts
    issued = []

    def arrive(index):
        _, _, landing, _, _, rows_sent = phases[index]
        drain(landing.at[pl.ds(0, (n - 1) * rows_sent)], w_recv.at[index])
        ahead = index + (WINDOW if index < first else LATE_WINDOW)
        while len(issued) <= min(ahead, len(phases) - 1):
            send(len(issued))
            issued.append(len(issued))

    def swap(buffer, slot):
        copies = []
        for step in range(1, cores):
            copies.append(
                pltpu.make_async_remote_copy(
                    src_ref=buffer, dst_ref=buffer,
                    send_sem=tp_send.at[slot, step - 1], recv_sem=tp_recv.at[slot, step - 1],
                    device_id={"tp": lax.rem(core + step, cores)}, device_id_type=MESH,
                )
            )
        for copy in copies:
            copy.start()
        return copies

    cast(0)
    loads[0].wait()
    values = tok_raw[...].astype(jnp.float32)
    square[core] = jnp.broadcast_to(jnp.sum(values * values, axis=1, keepdims=True), square.shape[1:])
    pl.semaphore_wait(barrier, n - 1 + cores - 1)
    send(0)
    issued.append(0)
    swapped = swap(square.at[core], 0)

    loads[2].wait()
    loads[3].wait()
    names = lax.broadcasted_iota(jnp.int32, (n, tok_rows), 0)
    weight = jnp.zeros((n, tok_rows), jnp.float32)
    member = jnp.zeros((n, tok_rows), jnp.float32)
    for k in range(top_count):
        hit = jnp.broadcast_to(routes_v[k:k + 1, :], (n, tok_rows)) == names
        weight = weight + jnp.where(hit, jnp.broadcast_to(weights_v[k:k + 1, :], (n, tok_rows)), 0.0)
        member = member + jnp.where(hit, 1.0, 0.0)
    before = lax.broadcasted_iota(jnp.int32, (tok_rows, tok_rows), 0)
    after = lax.broadcasted_iota(jnp.int32, (tok_rows, tok_rows), 1)
    earlier = jnp.where(before < after, 1.0, 0.0).astype(jnp.bfloat16)
    place = jnp.dot(member.astype(jnp.bfloat16), earlier, preferred_element_type=jnp.float32)
    place = jnp.where(member > 0.0, place, -1.0)
    for p in range(depths):
        info[z, 0, p] = weight[p * plane:(p + 1) * plane]
        info[z, 1, p] = place[p * plane:(p + 1) * plane]

    for copy in swapped:
        copy.wait()
    total = square[0]
    for part in range(1, cores):
        total = total + square[part]
    scale = lax.rsqrt(total / (width * cores) + epsilon)
    values = tok_raw[...].astype(jnp.float32)
    scale = jnp.concatenate([scale] * (width // scale.shape[1]), axis=1)
    block[z] = (values * scale).astype(jnp.bfloat16)

    def give_tokens(dest, received):
        remote(block.at[z], block.at[z], t_send.at[0], received.at[0], fs(dest * plane + q))
        remote(info.at[z], info.at[z], t_send.at[1], received.at[1], fs(dest * plane + q))

    give_tokens(other_leader, far_recv)
    for step in range(1, half):
        give_tokens(base + lax.rem(place_in_half + step, half), near_recv)
    for index in range(1, min(WINDOW, len(phases))):
        cast(index)
        send(index)
        issued.append(index)
    for index in range(WINDOW, len(phases)):
        cast(index)

    def take_far():
        drain(block.at[pl.ds(0, half)], far_recv.at[0])
        drain(info.at[pl.ds(0, half)], far_recv.at[1])

    def forward():
        @pl.when(z == leader)
        def _():
            take_far()
            for step in range(1, half):
                dest = fs((base + lax.rem(place_in_half + step, half)) * plane + q)
                remote(block.at[pl.ds(other, half)], block.at[pl.ds(other, half)], fwd_send.at[0], far_recv.at[0], dest)
                remote(info.at[pl.ds(other, half)], info.at[pl.ds(other, half)], fwd_send.at[1], far_recv.at[1], dest)

    slices = picked.shape[0]
    slice_width = width // slices
    own_picks = [
        pltpu.make_async_copy(picked.at[f, q], rows.at[core, f, q], own_sem.at[f]) for f in range(slices)
    ]

    def choose(source):
        slot = lax.broadcasted_iota(jnp.int32, (items, tok_rows), 0).astype(jnp.float32)
        weights = info[source, 0, z]
        places = info[source, 1, z]
        chosen, mixing = [], []
        for j in range(plane):
            at = jnp.broadcast_to(places[j:j + 1, :], (items, tok_rows)) == slot
            chosen.append(jnp.where(at, 1.0, 0.0))
            mixing.append(jnp.where(at, jnp.broadcast_to(weights[j:j + 1, :], (items, tok_rows)), 0.0))
        picks[...] = jnp.concatenate(chosen, axis=0).astype(jnp.bfloat16)
        mix = jnp.concatenate(mixing, axis=0).T
        high = mix.astype(jnp.bfloat16)
        mix_high[source] = high
        mix_low[source] = (mix - high.astype(jnp.float32)).astype(jnp.bfloat16)

    def dispatch(turn, f):
        if turn < half:
            source = base + lax.rem(place_in_half + turn, half)
        else:
            source = other + (turn - half)
        if f == 0:
            if turn == 1:
                drain(block.at[pl.ds(0, half - 1)], near_recv.at[0])
                drain(info.at[pl.ds(0, half - 1)], near_recv.at[1])
            if turn == half:
                @pl.when(z != leader)
                def _():
                    take_far()
            choose(source)
        part = block[source, :, f * slice_width:(f + 1) * slice_width]
        outbound = jnp.dot(picks[...], part, preferred_element_type=jnp.float32).astype(jnp.bfloat16)
        for j in range(plane):
            picked[f, j, source] = outbound[j * items:(j + 1) * items]
        for step in range(1, plane):
            peer = lax.rem(q + step, plane)
            remote(
                picked.at[f, peer, source], rows.at[core, f, q, source],
                p_send.at[f], p_recv.at[f], fs(z * plane + peer),
            )
        if turn == depths - 1:
            own_picks[f].start()

    swaps = []

    def collect():
        for f in range(slices):
            drain(rows.at[core, f, pl.ds(0, plane - 1)], p_recv.at[f])
            own_picks[f].wait()
        swaps.extend(swap(rows.at[core], 1))

    steps = [(0, dispatch, (0, 0))]
    for turn in range(depths):
        for f in range(slices):
            if turn + f > 0:
                at = turn * slices + f if turn < half else FAR_AT + (turn - half) * slices + f
                steps.append((at, dispatch, (turn, f)))
    at_far = next(i for i, (_, _, what) in enumerate(steps) if what[0] == half)
    steps.insert(at_far, (FORWARD_AT, forward, ()))
    steps.append((COLLECT_AT, collect, ()))
    tasks = {}
    for at, task, what in steps:
        tasks.setdefault(min(at, first - 1), []).append((task, what))
    tile = depths * items

    def first_layer(p):
        def one(group, carry):
            both = jnp.zeros((tile, 2 * lanes), jnp.float32)
            for part in range(cores):
                taken = jnp.concatenate([rows[part, f, group].reshape(tile, slice_width) for f in range(slices)], axis=1)
                both = both + jnp.dot(taken, pair[p, pl.ds(part * width, width), :], preferred_element_type=jnp.float32)
            hidden[core, p, group] = activate(both[:, :lanes], both[:, lanes:]).astype(jnp.bfloat16)
            return carry

        lax.fori_loop(0, plane, one, 0)
        swaps.extend(swap(hidden.at[core, p], 2 + p))

    computed = 0
    for index in range(first):
        arrive(index)
        for task, what in tasks.get(index, ()):
            task(*what)
        if index > COLLECT_AT or index == first - 1:
            if computed == 0:
                while swaps:
                    swaps.pop().wait()
            while (computed + 1) * parts <= index + 1:
                first_layer(computed)
                computed += 1

    def direct(c):
        return c >= chunks - DIRECT

    def expert(c):
        arrive(first + c)
        while swaps:
            swaps.pop(0).wait()

        def second_layer(group):
            summed = jnp.zeros((tile, chunk), jnp.float32)
            for part in range(cores):
                units_in = jnp.concatenate([hidden[part, p, group] for p in range(pieces)], axis=1)
                summed = summed + jnp.dot(
                    units_in, down[c, pl.ds(part * columns, columns), :], preferred_element_type=jnp.float32
                )
            return summed.astype(jnp.bfloat16).reshape(depths, items, chunk)

        def give(peer, start, which):
            at = pl.ds(start, half)
            remote(
                results.at[c, peer, at], back.at[c, q, at],
                r_send.at[c, which], r_recv.at[c, which], fs(z * plane + peer),
            )

        def far(step, carry):
            peer = lax.rem(q + step, plane)
            results[c, peer] = second_layer(peer)
            give(peer, other, 0)
            return carry

        def near(step, carry):
            give(lax.rem(q + step, plane), base, 1)
            return carry

        lax.fori_loop(1, plane, far, 0)
        lax.fori_loop(1, plane, near, 0)
        back[c, q] = second_layer(q)

    def relay(c):
        def mix(target):
            data = back[c, :, target].reshape(plane * items, chunk)
            summed = jnp.dot(mix_high[target], data, preferred_element_type=jnp.float32)
            summed = summed + jnp.dot(mix_low[target], data, preferred_element_type=jnp.float32)
            part_f[c, target] = summed
            part_s[c, target] = summed.astype(jnp.bfloat16)

        def far(k, carry):
            mix(other + k)
            return carry

        def near(k, carry):
            mix(base + lax.rem(place_in_half + k, half))
            return carry

        drain(back.at[c, pl.ds(0, plane - 1), pl.ds(0, half)], r_recv.at[c, 0])
        lax.fori_loop(0, half, far, 0)

        if direct(c):
            for k in range(half):
                remote(
                    part_s.at[c, other + k], cross_in.at[c, place_in_half],
                    x_send.at[c], x_recv.at[c], fs((other + k) * plane + q),
                )
        else:
            @pl.when(z != leader)
            def _():
                remote(
                    part_s.at[c, pl.ds(other, half)], lead_in.at[c, place_in_half],
                    l_send.at[c], l_recv.at[c], fs(leader * plane + q),
                )

        drain(back.at[c, pl.ds(0, plane - 1), pl.ds(0, half)], r_recv.at[c, 1])
        lax.fori_loop(0, half, near, 0)
        for step in range(1, half):
            target = base + lax.rem(place_in_half + step, half)
            remote(
                part_s.at[c, target], half_in.at[c, place_in_half],
                h_send.at[c], h_recv.at[c], fs(target * plane + q),
            )

    def lead(c):
        if direct(c):
            return

        @pl.when(z == leader)
        def _():
            if half > 1:
                drain(lead_in.at[c, pl.ds(0, half - 1)], l_recv.at[c])
            for k in range(half):
                summed = part_f[c, other + k]
                for step in range(1, half):
                    summed = summed + lead_in[c, lax.rem(place_in_half + step, half), k].astype(jnp.float32)
                cross[c, k] = summed.astype(jnp.bfloat16)
            for k in range(half):
                remote(cross.at[c, k], cross_in.at[c, 0], x_send.at[c], x_recv.at[c], fs((other + k) * plane + q))

    def finish(c):
        summed = part_f[c, z]
        if half > 1:
            drain(half_in.at[c, pl.ds(0, half - 1)], h_recv.at[c])
            for step in range(1, half):
                summed = summed + half_in[c, lax.rem(place_in_half + step, half)].astype(jnp.float32)
        taken = half if direct(c) else 1
        drain(cross_in.at[c, pl.ds(0, taken)], x_recv.at[c])
        for k in range(taken):
            summed = summed + cross_in[c, k].astype(jnp.float32)
        mixed[:, c * chunk:(c + 1) * chunk] = summed.astype(jnp.bfloat16)

    stages = ((relay, RELAY_LAG), (lead, LEAD_LAG), (finish, END_LAG))
    done = [0, 0, 0]
    for c in range(chunks):
        expert(c)
        for stage, (task, lag) in enumerate(stages):
            if c >= lag:
                task(done[stage])
                done[stage] += 1
    for index, phase in enumerate(phases):
        drain(phase[1].at[pl.ds(0, n - 1)], w_send.at[index])
    drain(block.at[pl.ds(0, half)], t_send.at[0])
    drain(info.at[pl.ds(0, half)], t_send.at[1])
    for f in range(slices):
        drain(picked.at[f, pl.ds(0, plane - 1)], p_send.at[f])

    @pl.when(z == leader)
    def _():
        for step in range(1, half):
            drain(block.at[pl.ds(0, half)], fwd_send.at[0])
            drain(info.at[pl.ds(0, half)], fwd_send.at[1])

    while done[0] < chunks:
        relay(done[0])
        done[0] += 1
        if done[1] < done[0] - 1:
            lead(done[1])
            done[1] += 1
    for c in range(done[1], chunks):
        lead(c)

    for c in range(chunks):
        for which in range(2):
            drain(results.at[c, pl.ds(0, plane - 1), pl.ds(0, half)], r_send.at[c, which])
        if half > 1:
            drain(part_s.at[c, pl.ds(0, half - 1)], h_send.at[c])
        if direct(c):
            drain(part_s.at[c, pl.ds(0, half)], x_send.at[c])

    @pl.when(z == leader)
    def _():
        for c in range(chunks):
            if not direct(c):
                drain(cross.at[c], x_send.at[c])

    @pl.when(z != leader)
    def _():
        for c in range(chunks):
            if not direct(c):
                drain(part_s.at[c, pl.ds(0, half)], l_send.at[c])

    for c in range(done[2], chunks):
        finish(c)


def place(mixed, pair, down, mixed_out, gate_out, up_out, down_out, sem):
    pieces, _, both = pair.shape
    chunks, _, chunk = down.shape
    lanes = both // 2
    moves = [(mixed, mixed_out)]
    for p in range(pieces):
        at = pl.ds(p * lanes, lanes)
        moves.append((pair.at[p, :, pl.ds(0, lanes)], gate_out.at[:, at]))
        moves.append((pair.at[p, :, pl.ds(lanes, lanes)], up_out.at[:, at]))
    for c in range(chunks):
        moves.append((down.at[c], down_out.at[:, pl.ds(c * chunk, chunk)]))
    copies = [pltpu.make_async_copy(source, landing, sem.at[i]) for i, (source, landing) in enumerate(moves)]
    for copy in copies:
        copy.start()
    for copy in copies:
        copy.wait()


def shards(n, cores, tokens, norm_gain, gate_weight, up_weight, down_weight, routes, route_weights):
    experts, depth, columns = gate_weight.shape
    units, width = down_weight.shape[1:]
    tok_rows, top_count = routes.shape
    items = 2 * tok_rows * top_count // experts
    plane = plane_size(n)
    depths = n // plane
    half = depths // 2
    parts = max(1, min(PARTS, depth // 16))
    lanes = min(128, columns)
    pieces = columns // lanes
    chunk = max(128, width // CHUNKS)
    chunks = width // chunk
    slices = 2 if width % 256 == 0 else 1
    bf16, f32, dma = jnp.bfloat16, jnp.float32, pltpu.SemaphoreType.DMA
    phases = pieces * parts + chunks

    arrays = tokens, norm_gain.reshape(1, depth), gate_weight, up_weight, down_weight, routes.T, route_weights.T
    anywhere = pl.BlockSpec(memory_space=pl.ANY)
    near = pl.BlockSpec(memory_space=pltpu.VMEM)
    results = pl.pallas_call(
        functools.partial(kernel, n, cores, items, parts, chunks),
        out_shape=(
            jax.ShapeDtypeStruct((tok_rows, width), bf16),
            jax.ShapeDtypeStruct((pieces, n * depth, 2 * lanes), bf16),
            jax.ShapeDtypeStruct((chunks, n * units, chunk), bf16),
        ),
        in_specs=[anywhere] * 7,
        out_specs=(near,) * 3,
        scratch_shapes=[
            pltpu.VMEM((tok_rows, width), bf16),
            pltpu.VMEM((1, depth), f32),
            pltpu.VMEM((depth, lanes), f32),
            pltpu.VMEM((top_count, tok_rows), jnp.int32),
            pltpu.VMEM((top_count, tok_rows), f32),
            pltpu.VMEM((cores, tok_rows, lanes), f32),
            pltpu.VMEM((pieces, parts, n, depth // parts, lanes), f32),
            pltpu.VMEM((pieces, parts, n, depth // parts, lanes), f32),
            pltpu.VMEM((chunks, n, units, chunk), f32),
            pltpu.VMEM((pieces, parts, n, depth // parts, 2 * lanes), bf16),
            pltpu.VMEM((chunks, n, units, chunk), bf16),
            pltpu.VMEM((depths, tok_rows, width), bf16),
            pltpu.VMEM((depths, 2, depths, plane, tok_rows), f32),
            pltpu.VMEM((plane * items, tok_rows), bf16),
            pltpu.VMEM((depths, tok_rows, plane * items), bf16),
            pltpu.VMEM((depths, tok_rows, plane * items), bf16),
            pltpu.VMEM((slices, plane, depths, items, width // slices), bf16),
            pltpu.VMEM((cores, slices, plane, depths, items, width // slices), bf16),
            pltpu.VMEM((cores, pieces, plane, depths * items, lanes), bf16),
            pltpu.VMEM((chunks, plane, depths, items, chunk), bf16),
            pltpu.VMEM((chunks, plane, depths, items, chunk), bf16),
            pltpu.VMEM((chunks, depths, tok_rows, chunk), f32),
            pltpu.VMEM((chunks, depths, tok_rows, chunk), bf16),
            pltpu.VMEM((chunks, half, half, tok_rows, chunk), bf16),
            pltpu.VMEM((chunks, half, tok_rows, chunk), bf16),
            pltpu.VMEM((chunks, half, tok_rows, chunk), bf16),
            pltpu.VMEM((chunks, half, tok_rows, chunk), bf16),
            dma((4 + phases, 2)),
            dma((phases,)),
            dma((phases,)),
            dma((2,)),
            dma((2,)),
            dma((2,)),
            dma((2,)),
            dma((slices,)),
            dma((slices,)),
            dma((slices,)),
            dma((2 + pieces, max(1, cores - 1))),
            dma((2 + pieces, max(1, cores - 1))),
            dma((chunks, 2)),
            dma((chunks, 2)),
            dma((chunks,)),
            dma((chunks,)),
            dma((chunks,)),
            dma((chunks,)),
            dma((chunks,)),
            dma((chunks,)),
        ],
        compiler_params=pltpu.CompilerParams(
            collective_id=0, has_side_effects=True, vmem_limit_bytes=44 * 1024 * 1024
        ),
    )(*(pltpu.with_memory_space_constraint(array, pltpu.HBM) for array in arrays))
    ready = (tok_rows, width), (n * depth, columns), (n * depth, columns), (n * units, width)
    mixed, gate_ready, up_ready, down_ready = pl.pallas_call(
        place,
        out_shape=tuple(jax.ShapeDtypeStruct(shape, bf16) for shape in ready),
        in_specs=[anywhere] * 3,
        out_specs=(anywhere,) * 4,
        scratch_shapes=[dma((1 + 2 * pieces + chunks,))],
        compiler_params=pltpu.CompilerParams(vmem_limit_bytes=1024 * 1024),
    )(*results)
    return (mixed, gate_ready[None], up_ready[None], down_ready[None])


def solution(mesh):
    placed = (
        P("fs", "tp"),
        P("fs"),
        P(None, "fs", "tp"),
        P(None, "fs", "tp"),
        P(None, "fs", "tp"),
        P("fs", None),
        P("fs", None),
    )
    return jax.shard_map(
        functools.partial(shards, mesh.shape["fs"], mesh.shape["tp"]),
        mesh=mesh,
        in_specs=placed,
        out_specs=(P("fs", "tp"), P("fs", None, "tp"), P("fs", None, "tp"), P("fs", None, "tp")),
        check_vma=False,
    )
```

```python
import functools
import math

import jax
import jax.numpy as jnp
from jax import lax
from jax.experimental import pallas as pl
from jax.experimental.pallas import tpu as pltpu
from jax.sharding import PartitionSpec as P

epsilon = 1e-05
MESH = pl.DeviceIdType.MESH
CHUNKS = 8
PARTS = 4
WINDOW, LATE_WINDOW = 4, 4
RELAY_LAG, LEAD_LAG, END_LAG = 2, 4, 7
DIRECT = 1
EARLY_AT = 5
NEAR_AT, FORWARD_AT, FAR_AT, COLLECT_AT = 2, 2, 7, 12


def activate(gate_pre, up_pre):
    gated = jnp.minimum(gate_pre, 7.0)
    upper = jnp.clip(up_pre, -7.0, 7.0)
    return (upper + 1.0) * gated * jax.nn.sigmoid(1.702 * gated)


def plane_size(n):
    return max(size for size in range(1, math.isqrt(n) + 1) if n % size == 0 and (n // size) % 2 == 0)


def kernel(
    n, cores, items, parts, chunks,
    tokens_in, gain_in, gate_in, up_in, down_in, routes_in, weights_in,
    mixed, pair, down,
    tok_raw, gain_row, gain_tile, routes_v, weights_v, square,
    gate_f, up_f, down_f, pair_s, down_s,
    block, info, picks, mix_high, mix_low, picked, rows, hidden,
    results, back, part_f, part_s, lead_in, half_in, cross, cross_in,
    load_sem, w_send, w_recv, t_send, near_recv, far_recv, fwd_send, p_send, p_recv, own_sem, tp_send, tp_recv,
    r_send, r_recv, h_send, h_recv, l_send, l_recv, x_send, x_recv,
):
    me = lax.axis_index("fs")
    core = lax.axis_index("tp")
    plane = plane_size(n)
    depths = n // plane
    half = depths // 2
    z = me // plane
    q = lax.rem(me, plane)
    base = (z // half) * half
    other = half - base
    leader = half - 1 + z // half
    other_leader = half - z // half
    place_in_half = z - base

    tok_rows, width = tokens_in.shape
    depth, columns = gate_in.shape[1:]
    units = down_in.shape[1]
    pieces = pair.shape[0]
    lanes = columns // pieces
    size = depth // parts
    chunk = width // chunks
    top_count = routes_in.shape[0]

    def fs(index):
        return {"fs": index}

    def remote(source, landing, sent, received, where):
        pltpu.make_async_remote_copy(
            src_ref=source, dst_ref=landing, send_sem=sent, recv_sem=received,
            device_id=where, device_id_type=MESH,
        ).start()

    def drain(ref, semaphore):
        pltpu.make_async_copy(ref, ref, semaphore).wait()

    barrier = pltpu.get_barrier_semaphore()

    def greet(step, carry):
        pl.semaphore_signal(barrier, inc=1, device_id=fs(lax.rem(me + step, n)), device_id_type=MESH)
        return carry

    lax.fori_loop(1, n, greet, 0)
    for step in range(1, cores):
        pl.semaphore_signal(barrier, inc=1, device_id={"tp": lax.rem(core + step, cores)}, device_id_type=MESH)

    small = ((tokens_in, tok_raw), (gain_in, gain_row), (routes_in, routes_v), (weights_in, weights_v))
    loads = [pltpu.make_async_copy(source, landing, load_sem.at[i, 0]) for i, (source, landing) in enumerate(small)]
    phases = []
    for p in range(pieces):
        for r in range(parts):
            at = pl.ds(r * size, size), pl.ds(p * lanes, lanes)
            sources = ((gate_in.at[:, at[0], at[1]], gate_f.at[p, r]), (up_in.at[:, at[0], at[1]], up_f.at[p, r]))
            phases.append((sources, pair_s.at[p, r], pair.at[p], depth, r * size, size))
    for c in range(chunks):
        sources = ((down_in.at[:, :, pl.ds(c * chunk, chunk)], down_f.at[c]),)
        phases.append((sources, down_s.at[c], down.at[c], units, 0, units))
    weight_loads = []
    for phase in phases:
        at = len(small) + len(weight_loads)
        weight_loads.append([
            pltpu.make_async_copy(source, landing, load_sem.at[at, i]) for i, (source, landing) in enumerate(phase[0])
        ])
    loads[1].start()
    for copy in weight_loads[0]:
        copy.start()
    for at in (0, 2, 3):
        loads[at].start()
    for copies in weight_loads[1:]:
        for copy in copies:
            copy.start()

    loads[1].wait()
    row_at = lax.broadcasted_iota(jnp.int32, (depth, depth), 0)
    lane_at = lax.broadcasted_iota(jnp.int32, (depth, depth), 1)
    spread = jnp.where(row_at == lane_at, jnp.broadcast_to(gain_row[...], (depth, depth)), 0.0)
    gain_tile[...] = jnp.broadcast_to(jnp.sum(spread, axis=1, keepdims=True), gain_tile.shape)

    def cast(index):
        sources, sent, landing, stride, offset, rows_sent = phases[index]
        for copy in weight_loads[index]:
            copy.wait()

        def rounded(peer):
            if len(sources) == 1:
                return sources[0][1][peer].astype(jnp.bfloat16)
            gain = gain_tile[offset:offset + rows_sent, :]
            return jnp.concatenate([(staged[peer] * gain).astype(jnp.bfloat16) for _, staged in sources], axis=1)

        def one(step, carry):
            peer = lax.rem(me + step, n)
            sent[peer] = rounded(peer)
            return carry

        lax.fori_loop(1, n, one, 0)
        landing[pl.ds(pl.multiple_of(me * stride + offset, rows_sent), rows_sent), :] = rounded(me)

    first = pieces * parts

    def send(index):
        _, sent, landing, stride, offset, rows_sent = phases[index]

        def to(peer, landing, sent, which, at):
            remote(sent.at[peer], landing.at[at], w_send.at[which], w_recv.at[which], fs(peer))

        def whole(step, carry):
            at = pl.ds(pl.multiple_of(me * stride + offset, rows_sent), rows_sent)
            to(lax.rem(me + step, n), landing, sent, index, at)
            return carry

        def beyond(step, carry):
            at = pl.ds(pl.multiple_of(me * stride + offset, rows_sent), rows_sent)
            to(other * plane + lax.rem(me + step, half * plane), landing, sent, index, at)
            return carry

        if index < first:
            lax.fori_loop(1, n, whole, 0)
        else:
            lax.fori_loop(0, half * plane, beyond, 0)
        for c in range(chunks):
            if index == min(EARLY_AT + c, first - 1):
                _, early_sent, early_landing, early_stride, _, early_rows = phases[first + c]
                at = pl.ds(pl.multiple_of(me * early_stride, early_rows), early_rows)
                for step in range(1, half * plane):
                    peer = base * plane + lax.rem(me - base * plane + step, half * plane)
                    to(peer, early_landing, early_sent, first + c, at)

    issued = []

    def arrive(index):
        _, _, landing, _, _, rows_sent = phases[index]
        drain(landing.at[pl.ds(0, (n - 1) * rows_sent)], w_recv.at[index])
        ahead = index + (WINDOW if index < first else LATE_WINDOW)
        while len(issued) <= min(ahead, len(phases) - 1):
            send(len(issued))
            issued.append(len(issued))

    def swap(buffer, slot):
        copies = []
        for step in range(1, cores):
            copies.append(
                pltpu.make_async_remote_copy(
                    src_ref=buffer, dst_ref=buffer,
                    send_sem=tp_send.at[slot, step - 1], recv_sem=tp_recv.at[slot, step - 1],
                    device_id={"tp": lax.rem(core + step, cores)}, device_id_type=MESH,
                )
            )
        for copy in copies:
            copy.start()
        return copies

    cast(0)
    loads[0].wait()
    values = tok_raw[...].astype(jnp.float32)
    square[core] = jnp.broadcast_to(jnp.sum(values * values, axis=1, keepdims=True), square.shape[1:])
    pl.semaphore_wait(barrier, n - 1 + cores - 1)
    send(0)
    issued.append(0)
    swapped = swap(square.at[core], 0)

    loads[2].wait()
    loads[3].wait()
    names = lax.broadcasted_iota(jnp.int32, (n, tok_rows), 0)
    weight = jnp.zeros((n, tok_rows), jnp.float32)
    member = jnp.zeros((n, tok_rows), jnp.float32)
    for k in range(top_count):
        hit = jnp.broadcast_to(routes_v[k:k + 1, :], (n, tok_rows)) == names
        weight = weight + jnp.where(hit, jnp.broadcast_to(weights_v[k:k + 1, :], (n, tok_rows)), 0.0)
        member = member + jnp.where(hit, 1.0, 0.0)
    before = lax.broadcasted_iota(jnp.int32, (tok_rows, tok_rows), 0)
    after = lax.broadcasted_iota(jnp.int32, (tok_rows, tok_rows), 1)
    earlier = jnp.where(before < after, 1.0, 0.0).astype(jnp.bfloat16)
    place = jnp.dot(member.astype(jnp.bfloat16), earlier, preferred_element_type=jnp.float32)
    place = jnp.where(member > 0.0, place, -1.0)
    for p in range(depths):
        info[z, 0, p] = weight[p * plane:(p + 1) * plane]
        info[z, 1, p] = place[p * plane:(p + 1) * plane]

    for copy in swapped:
        copy.wait()
    total = square[0]
    for part in range(1, cores):
        total = total + square[part]
    scale = lax.rsqrt(total / (width * cores) + epsilon)
    values = tok_raw[...].astype(jnp.float32)
    scale = jnp.concatenate([scale] * (width // scale.shape[1]), axis=1)
    block[z] = (values * scale).astype(jnp.bfloat16)

    def give_tokens(dest, received):
        remote(block.at[z], block.at[z], t_send.at[0], received.at[0], fs(dest * plane + q))
        remote(info.at[z], info.at[z], t_send.at[1], received.at[1], fs(dest * plane + q))

    give_tokens(other_leader, far_recv)
    for step in range(1, half):
        give_tokens(base + lax.rem(place_in_half + step, half), near_recv)
    for index in range(1, min(WINDOW, len(phases))):
        cast(index)
        send(index)
        issued.append(index)
    for index in range(WINDOW, len(phases)):
        cast(index)

    def take_far():
        drain(block.at[pl.ds(0, half)], far_recv.at[0])
        drain(info.at[pl.ds(0, half)], far_recv.at[1])

    def forward():
        @pl.when(z == leader)
        def _():
            take_far()
            for step in range(1, half):
                dest = fs((base + lax.rem(place_in_half + step, half)) * plane + q)
                remote(block.at[pl.ds(other, half)], block.at[pl.ds(other, half)], fwd_send.at[0], far_recv.at[0], dest)
                remote(info.at[pl.ds(other, half)], info.at[pl.ds(other, half)], fwd_send.at[1], far_recv.at[1], dest)

    slices = picked.shape[0]
    slice_width = width // slices
    own_picks = [
        pltpu.make_async_copy(picked.at[f, q], rows.at[core, f, q], own_sem.at[f]) for f in range(slices)
    ]

    def choose(source):
        slot = lax.broadcasted_iota(jnp.int32, (items, tok_rows), 0).astype(jnp.float32)
        weights = info[source, 0, z]
        places = info[source, 1, z]
        chosen, mixing = [], []
        for j in range(plane):
            at = jnp.broadcast_to(places[j:j + 1, :], (items, tok_rows)) == slot
            chosen.append(jnp.where(at, 1.0, 0.0))
            mixing.append(jnp.where(at, jnp.broadcast_to(weights[j:j + 1, :], (items, tok_rows)), 0.0))
        picks[...] = jnp.concatenate(chosen, axis=0).astype(jnp.bfloat16)
        mix = jnp.concatenate(mixing, axis=0).T
        high = mix.astype(jnp.bfloat16)
        mix_high[source] = high
        mix_low[source] = (mix - high.astype(jnp.float32)).astype(jnp.bfloat16)

    def dispatch(turn, f):
        if turn < half:
            source = base + lax.rem(place_in_half + turn, half)
        else:
            source = other + (turn - half)
        if f == 0:
            if turn == 1:
                drain(block.at[pl.ds(0, half - 1)], near_recv.at[0])
                drain(info.at[pl.ds(0, half - 1)], near_recv.at[1])
            if turn == half:
                @pl.when(z != leader)
                def _():
                    take_far()
            choose(source)
        part = block[source, :, f * slice_width:(f + 1) * slice_width]
        outbound = jnp.dot(picks[...], part, preferred_element_type=jnp.float32).astype(jnp.bfloat16)
        for j in range(plane):
            picked[f, j, source] = outbound[j * items:(j + 1) * items]
        for step in range(1, plane):
            peer = lax.rem(q + step, plane)
            remote(
                picked.at[f, peer, source], rows.at[core, f, q, source],
                p_send.at[f], p_recv.at[f], fs(z * plane + peer),
            )
        if turn == depths - 1:
            own_picks[f].start()

    swaps = []

    def collect():
        for f in range(slices):
            drain(rows.at[core, f, pl.ds(0, plane - 1)], p_recv.at[f])
            own_picks[f].wait()
        swaps.extend(swap(rows.at[core], 1))

    steps = [(0, dispatch, (0, 0))]
    for turn in range(depths):
        for f in range(slices):
            if turn + f > 0:
                at = turn * slices + f if turn < half else FAR_AT + (turn - half) * slices + f
                steps.append((at, dispatch, (turn, f)))
    at_far = next(i for i, (_, _, what) in enumerate(steps) if what[0] == half)
    steps.insert(at_far, (FORWARD_AT, forward, ()))
    steps.append((COLLECT_AT, collect, ()))
    tasks = {}
    for at, task, what in steps:
        tasks.setdefault(min(at, first - 1), []).append((task, what))
    tile = depths * items

    def first_layer(p):
        def one(group, carry):
            both = jnp.zeros((tile, 2 * lanes), jnp.float32)
            for part in range(cores):
                taken = jnp.concatenate([rows[part, f, group].reshape(tile, slice_width) for f in range(slices)], axis=1)
                both = both + jnp.dot(taken, pair[p, pl.ds(part * width, width), :], preferred_element_type=jnp.float32)
            hidden[core, p, group] = activate(both[:, :lanes], both[:, lanes:]).astype(jnp.bfloat16)
            return carry

        lax.fori_loop(0, plane, one, 0)
        swaps.extend(swap(hidden.at[core, p], 2 + p))

    computed = 0
    for index in range(first):
        arrive(index)
        for task, what in tasks.get(index, ()):
            task(*what)
        if index > COLLECT_AT or index == first - 1:
            if computed == 0:
                while swaps:
                    swaps.pop().wait()
            while (computed + 1) * parts <= index + 1:
                first_layer(computed)
                computed += 1

    def direct(c):
        return c >= chunks - DIRECT

    def expert(c):
        arrive(first + c)
        while swaps:
            swaps.pop(0).wait()

        def second_layer(group):
            summed = jnp.zeros((tile, chunk), jnp.float32)
            for part in range(cores):
                units_in = jnp.concatenate([hidden[part, p, group] for p in range(pieces)], axis=1)
                summed = summed + jnp.dot(
                    units_in, down[c, pl.ds(part * columns, columns), :], preferred_element_type=jnp.float32
                )
            return summed.astype(jnp.bfloat16).reshape(depths, items, chunk)

        def give(peer, start, which):
            at = pl.ds(start, half)
            remote(
                results.at[c, peer, at], back.at[c, q, at],
                r_send.at[c, which], r_recv.at[c, which], fs(z * plane + peer),
            )

        def far(step, carry):
            peer = lax.rem(q + step, plane)
            results[c, peer] = second_layer(peer)
            give(peer, other, 0)
            return carry

        def near(step, carry):
            give(lax.rem(q + step, plane), base, 1)
            return carry

        lax.fori_loop(1, plane, far, 0)
        lax.fori_loop(1, plane, near, 0)
        back[c, q] = second_layer(q)

    def relay(c):
        def mix(target):
            data = back[c, :, target].reshape(plane * items, chunk)
            summed = jnp.dot(mix_high[target], data, preferred_element_type=jnp.float32)
            summed = summed + jnp.dot(mix_low[target], data, preferred_element_type=jnp.float32)
            part_f[c, target] = summed
            part_s[c, target] = summed.astype(jnp.bfloat16)

        def far(k, carry):
            mix(other + k)
            return carry

        def near(k, carry):
            mix(base + lax.rem(place_in_half + k, half))
            return carry

        drain(back.at[c, pl.ds(0, plane - 1), pl.ds(0, half)], r_recv.at[c, 0])
        lax.fori_loop(0, half, far, 0)

        if direct(c):
            for k in range(half):
                remote(
                    part_s.at[c, other + k], cross_in.at[c, place_in_half],
                    x_send.at[c], x_recv.at[c], fs((other + k) * plane + q),
                )
        else:
            @pl.when(z != leader)
            def _():
                remote(
                    part_s.at[c, pl.ds(other, half)], lead_in.at[c, place_in_half],
                    l_send.at[c], l_recv.at[c], fs(leader * plane + q),
                )

        drain(back.at[c, pl.ds(0, plane - 1), pl.ds(0, half)], r_recv.at[c, 1])
        lax.fori_loop(0, half, near, 0)
        for step in range(1, half):
            target = base + lax.rem(place_in_half + step, half)
            remote(
                part_s.at[c, target], half_in.at[c, place_in_half],
                h_send.at[c], h_recv.at[c], fs(target * plane + q),
            )

    def lead(c):
        if direct(c):
            return

        @pl.when(z == leader)
        def _():
            if half > 1:
                drain(lead_in.at[c, pl.ds(0, half - 1)], l_recv.at[c])
            for k in range(half):
                summed = part_f[c, other + k]
                for step in range(1, half):
                    summed = summed + lead_in[c, lax.rem(place_in_half + step, half), k].astype(jnp.float32)
                cross[c, k] = summed.astype(jnp.bfloat16)
            for k in range(half):
                remote(cross.at[c, k], cross_in.at[c, 0], x_send.at[c], x_recv.at[c], fs((other + k) * plane + q))

    def finish(c):
        summed = part_f[c, z]
        if half > 1:
            drain(half_in.at[c, pl.ds(0, half - 1)], h_recv.at[c])
            for step in range(1, half):
                summed = summed + half_in[c, lax.rem(place_in_half + step, half)].astype(jnp.float32)
        taken = half if direct(c) else 1
        drain(cross_in.at[c, pl.ds(0, taken)], x_recv.at[c])
        for k in range(taken):
            summed = summed + cross_in[c, k].astype(jnp.float32)
        mixed[:, c * chunk:(c + 1) * chunk] = summed.astype(jnp.bfloat16)

    stages = ((relay, RELAY_LAG), (lead, LEAD_LAG), (finish, END_LAG))
    done = [0, 0, 0]
    for c in range(chunks):
        expert(c)
        for stage, (task, lag) in enumerate(stages):
            if c >= lag:
                task(done[stage])
                done[stage] += 1
    for index, phase in enumerate(phases):
        drain(phase[1].at[pl.ds(0, n - 1)], w_send.at[index])
    drain(block.at[pl.ds(0, half)], t_send.at[0])
    drain(info.at[pl.ds(0, half)], t_send.at[1])
    for f in range(slices):
        drain(picked.at[f, pl.ds(0, plane - 1)], p_send.at[f])

    @pl.when(z == leader)
    def _():
        for step in range(1, half):
            drain(block.at[pl.ds(0, half)], fwd_send.at[0])
            drain(info.at[pl.ds(0, half)], fwd_send.at[1])

    while done[0] < chunks:
        relay(done[0])
        done[0] += 1
        if done[1] < done[0] - 1:
            lead(done[1])
            done[1] += 1
    for c in range(done[1], chunks):
        lead(c)

    for c in range(chunks):
        for which in range(2):
            drain(results.at[c, pl.ds(0, plane - 1), pl.ds(0, half)], r_send.at[c, which])
        if half > 1:
            drain(part_s.at[c, pl.ds(0, half - 1)], h_send.at[c])
        if direct(c):
            drain(part_s.at[c, pl.ds(0, half)], x_send.at[c])

    @pl.when(z == leader)
    def _():
        for c in range(chunks):
            if not direct(c):
                drain(cross.at[c], x_send.at[c])

    @pl.when(z != leader)
    def _():
        for c in range(chunks):
            if not direct(c):
                drain(part_s.at[c, pl.ds(0, half)], l_send.at[c])

    for c in range(done[2], chunks):
        finish(c)


def place(mixed, pair, down, mixed_out, gate_out, up_out, down_out, sem):
    pieces, _, both = pair.shape
    chunks, _, chunk = down.shape
    lanes = both // 2
    moves = [(mixed, mixed_out)]
    for p in range(pieces):
        at = pl.ds(p * lanes, lanes)
        moves.append((pair.at[p, :, pl.ds(0, lanes)], gate_out.at[:, at]))
        moves.append((pair.at[p, :, pl.ds(lanes, lanes)], up_out.at[:, at]))
    for c in range(chunks):
        moves.append((down.at[c], down_out.at[:, pl.ds(c * chunk, chunk)]))
    copies = [pltpu.make_async_copy(source, landing, sem.at[i]) for i, (source, landing) in enumerate(moves)]
    for copy in copies:
        copy.start()
    for copy in copies:
        copy.wait()


def shards(n, cores, tokens, norm_gain, gate_weight, up_weight, down_weight, routes, route_weights):
    experts, depth, columns = gate_weight.shape
    units, width = down_weight.shape[1:]
    tok_rows, top_count = routes.shape
    items = 2 * tok_rows * top_count // experts
    plane = plane_size(n)
    depths = n // plane
    half = depths // 2
    parts = max(1, min(PARTS, depth // 16))
    lanes = min(128, columns)
    pieces = columns // lanes
    chunk = max(128, width // CHUNKS)
    chunks = width // chunk
    slices = 2 if width % 256 == 0 else 1
    bf16, f32, dma = jnp.bfloat16, jnp.float32, pltpu.SemaphoreType.DMA
    phases = pieces * parts + chunks

    arrays = tokens, norm_gain.reshape(1, depth), gate_weight, up_weight, down_weight, routes.T, route_weights.T
    anywhere = pl.BlockSpec(memory_space=pl.ANY)
    near = pl.BlockSpec(memory_space=pltpu.VMEM)
    results = pl.pallas_call(
        functools.partial(kernel, n, cores, items, parts, chunks),
        out_shape=(
            jax.ShapeDtypeStruct((tok_rows, width), bf16),
            jax.ShapeDtypeStruct((pieces, n * depth, 2 * lanes), bf16),
            jax.ShapeDtypeStruct((chunks, n * units, chunk), bf16),
        ),
        in_specs=[anywhere] * 7,
        out_specs=(near,) * 3,
        scratch_shapes=[
            pltpu.VMEM((tok_rows, width), bf16),
            pltpu.VMEM((1, depth), f32),
            pltpu.VMEM((depth, lanes), f32),
            pltpu.VMEM((top_count, tok_rows), jnp.int32),
            pltpu.VMEM((top_count, tok_rows), f32),
            pltpu.VMEM((cores, tok_rows, lanes), f32),
            pltpu.VMEM((pieces, parts, n, depth // parts, lanes), f32),
            pltpu.VMEM((pieces, parts, n, depth // parts, lanes), f32),
            pltpu.VMEM((chunks, n, units, chunk), f32),
            pltpu.VMEM((pieces, parts, n, depth // parts, 2 * lanes), bf16),
            pltpu.VMEM((chunks, n, units, chunk), bf16),
            pltpu.VMEM((depths, tok_rows, width), bf16),
            pltpu.VMEM((depths, 2, depths, plane, tok_rows), f32),
            pltpu.VMEM((plane * items, tok_rows), bf16),
            pltpu.VMEM((depths, tok_rows, plane * items), bf16),
            pltpu.VMEM((depths, tok_rows, plane * items), bf16),
            pltpu.VMEM((slices, plane, depths, items, width // slices), bf16),
            pltpu.VMEM((cores, slices, plane, depths, items, width // slices), bf16),
            pltpu.VMEM((cores, pieces, plane, depths * items, lanes), bf16),
            pltpu.VMEM((chunks, plane, depths, items, chunk), bf16),
            pltpu.VMEM((chunks, plane, depths, items, chunk), bf16),
            pltpu.VMEM((chunks, depths, tok_rows, chunk), f32),
            pltpu.VMEM((chunks, depths, tok_rows, chunk), bf16),
            pltpu.VMEM((chunks, half, half, tok_rows, chunk), bf16),
            pltpu.VMEM((chunks, half, tok_rows, chunk), bf16),
            pltpu.VMEM((chunks, half, tok_rows, chunk), bf16),
            pltpu.VMEM((chunks, half, tok_rows, chunk), bf16),
            dma((4 + phases, 2)),
            dma((phases,)),
            dma((phases,)),
            dma((2,)),
            dma((2,)),
            dma((2,)),
            dma((2,)),
            dma((slices,)),
            dma((slices,)),
            dma((slices,)),
            dma((2 + pieces, max(1, cores - 1))),
            dma((2 + pieces, max(1, cores - 1))),
            dma((chunks, 2)),
            dma((chunks, 2)),
            dma((chunks,)),
            dma((chunks,)),
            dma((chunks,)),
            dma((chunks,)),
            dma((chunks,)),
            dma((chunks,)),
        ],
        compiler_params=pltpu.CompilerParams(
            collective_id=0, has_side_effects=True, vmem_limit_bytes=44 * 1024 * 1024
        ),
    )(*(pltpu.with_memory_space_constraint(array, pltpu.HBM) for array in arrays))
    ready = (tok_rows, width), (n * depth, columns), (n * depth, columns), (n * units, width)
    mixed, gate_ready, up_ready, down_ready = pl.pallas_call(
        place,
        out_shape=tuple(jax.ShapeDtypeStruct(shape, bf16) for shape in ready),
        in_specs=[anywhere] * 3,
        out_specs=(anywhere,) * 4,
        scratch_shapes=[dma((1 + 2 * pieces + chunks,))],
        compiler_params=pltpu.CompilerParams(vmem_limit_bytes=1024 * 1024),
    )(*results)
    return (mixed, gate_ready[None], up_ready[None], down_ready[None])


def solution(mesh):
    placed = (
        P("fs", "tp"),
        P("fs"),
        P(None, "fs", "tp"),
        P(None, "fs", "tp"),
        P(None, "fs", "tp"),
        P("fs", None),
        P("fs", None),
    )
    return jax.shard_map(
        functools.partial(shards, mesh.shape["fs"], mesh.shape["tp"]),
        mesh=mesh,
        in_specs=placed,
        out_specs=(P("fs", "tp"), P("fs", None, "tp"), P("fs", None, "tp"), P("fs", None, "tp")),
        check_vma=False,
    )
```
